512 devices in a mesh: sp: 128 (over z, x, core), tp: 4 (over y).
Axes of the slice: x: 4, y: 4, z: 16, core: 2. Of those that a mesh axis runs over, the one named last changes fastest.
Arguments:
- tokens: bfloat16 [32768, 2048], P('sp'), may hold values from -6 to 6
- documents: int32 [32768], P('sp'), may hold values from 0 to 63, never falling along the last dimension, each value on 1 to 1024 neighbouring positions
- norm_gain: float32 [1, 2048], replicated, may hold values from 0.1 to 1.9
- w_query: bfloat16 [1, 2048, 2048], P(None, 'sp', 'tp'), may hold values from -0.125 to 0.125
- w_key: bfloat16 [1, 2048, 2048], P(None, 'sp', 'tp'), may hold values from -0.125 to 0.125
- w_value: bfloat16 [1, 2048, 2048], P(None, 'sp', 'tp'), may hold values from -0.125 to 0.125
- w_out: bfloat16 [1, 2048, 2048], P(None, None, 'sp'), may hold values from -0.59765625 to 0.59765625
- rel_bias: float32 [1, 32, 257], P(None, 'tp'), may hold values from -8 to 240
Outputs:
- mixed: bfloat16 [32768, 2048], P('sp')
The draws below stay inside these ranges and needn't reach their ends.
Inputs may be any that keep to these rules, and one draw needn't show every extreme that they name: `documents`: document numbers never fall along the sequence; a document has 1 to 1024 positions.
All inputs are finite; a program needn't handle non-finite values.
Results may differ from the reference program's by a relative error of at most 0.007.
Values may be sent and summed in bfloat16 or wider, within the bound.
No kernel may reach another device: no remote copies, remote signals or barrier semaphores. Data moves between devices by JAX's collectives and lax.ppermute only.
A program may use at most 128 MiB of HBM per device.

```python
import math
import jax
import jax.numpy as jnp
import numpy as np
from jax import lax

D = 2048
HEADS = 32
HEAD_DIM = 64
SEG = 64
LEFT = 4
REL_CLIP = 128
LAYERS = 1
TOK_DEV = 256
TOKENS = 32768
DOC_SPAN = 1024
N_SP = 128


def draw_rel_bias(key, part):
    bias_shape = (LAYERS, HEADS, 2 * REL_CLIP + 1)
    base_draw = jnp.clip(jax.random.normal(key, bias_shape, jnp.float32) * 1.5, -8.0, 8.0)
    return base_draw


def block_scale(key, dims, split, low, high):
    def one(dim, blocks):
        heights = jax.random.uniform(jax.random.fold_in(jax.random.fold_in(key, 6), dim), (blocks,), jnp.float32, low / len(split), high / len(split))
        return jnp.repeat(jnp.exp(heights), dims[dim] // blocks).reshape((-1,) + (1,) * (len(dims) - dim - 1))

    gain = one(*split[0])
    for cut in split[1:]:
        gain = gain * one(*cut)
    return gain


def profile(amount, total, bound, slope):
    portions = [(1 << 20) // math.isqrt(standing ** slope) + 1 for standing in range(2, amount + 1)]
    spare, holding = total - bound - (amount - 1), [1] * (amount - 1)
    while spare > 0:
        candidates = [i for i in range(amount - 1) if holding[i] < bound]
        mass, left = sum([portions[i] for i in candidates]), spare
        for i in candidates:
            addition = min(bound - holding[i], max(1, left * portions[i] // mass), spare)
            holding[i] = holding[i] + addition
            spare = spare - addition
    return np.array([bound] + holding)


def ragged_sizes(rng, number_of, total, limit, lean):
    if number_of == 2:
        one = jax.random.randint(rng, (), max(1, total - limit), min(limit, total - 1) + 1)
        return jnp.stack([one, total - one])
    lengths = jnp.asarray(profile(number_of, total, limit, lean), jnp.int32)
    pairs = (number_of - 1) // 2
    source_of, receiver = lengths[1:1 + 2 * pairs:2], lengths[2:2 + 2 * pairs:2]
    slack = jnp.minimum(source_of - 1, limit - receiver)
    passed = jax.random.randint(jax.random.fold_in(rng, 1), (pairs,), 0, 1 << 20) % (slack + 1)
    lengths = lengths.at[1:1 + 2 * pairs:2].set(source_of - passed).at[2:2 + 2 * pairs:2].set(receiver + passed)
    return lengths[jax.random.permutation(jax.random.fold_in(rng, 2), number_of)]


def normal_values(stream_key, extent, width, limit, shards=(), held_as=jnp.bfloat16):
    drawn = width * jax.random.normal(stream_key, extent, jnp.float32)
    if shards:
        drawn = drawn * block_scale(stream_key, extent, shards, -0.22, 0.18)
    return jnp.clip(drawn, -limit, limit).astype(held_as)


def setup_inputs(seed: int = 0) -> dict:
    keys = jax.random.split(jax.random.key(seed), 9)
    tokens = normal_values(keys[0], (TOKENS, D), 1.0, 6.0, ((0, 128),))
    documents = jnp.searchsorted(jnp.cumsum(ragged_sizes(keys[1], N_SP // 2, TOKENS, DOC_SPAN, 0)), jnp.arange(TOKENS), side="right").astype(jnp.int32)
    norm_gain = jnp.clip(1.0 + 0.18 * jax.random.normal(keys[2], (LAYERS, D), jnp.float32), 0.1, 1.9)
    w_query = normal_values(keys[3], (LAYERS, D, HEADS * HEAD_DIM), D ** -0.5, 0.125, ((1, 128), (2, 4)))
    w_key = normal_values(keys[4], (LAYERS, D, HEADS * HEAD_DIM), D ** -0.5, 0.125, ((1, 128), (2, 4)))
    w_value = normal_values(keys[5], (LAYERS, D, HEADS * HEAD_DIM), D ** -0.5, 0.125, ((1, 128), (2, 4)))
    w_out = normal_values(keys[6], (LAYERS, HEADS * HEAD_DIM, D), 0.1, 0.59765625, ((2, 128),))
    rel_bias = draw_rel_bias(jax.random.fold_in(keys[8], 71), 0)
    return dict(tokens=tokens, documents=documents, norm_gain=norm_gain, w_query=w_query, w_key=w_key, w_value=w_value, w_out=w_out, rel_bias=rel_bias)


EPS = 1e-06

def attend(queries, keys_all, values_all, query_pos, key_pos, query_doc, key_doc, bias_table):
    scores = jnp.einsum('qhe,khe->hqk', queries.astype(jnp.float32), keys_all.astype(jnp.float32)) * HEAD_DIM ** (-0.5)
    distance = jnp.clip(query_pos[:, None] - key_pos[None, :], -REL_CLIP, REL_CLIP) + REL_CLIP
    scores = scores + jnp.take(bias_table, distance, axis=1)
    query_seg = query_pos // SEG
    key_seg = key_pos // SEG
    allowed = (key_pos[None, :] >= 0) & (key_seg[None, :] <= query_seg[:, None]) & (key_seg[None, :] >= query_seg[:, None] - LEFT) & (key_doc[None, :] == query_doc[:, None])
    scores = jnp.where(allowed[None], scores, -1e+30)
    peak = lax.optimization_barrier(jnp.max(scores, axis=-1, keepdims=True))
    raised = jnp.exp(scores - peak)
    weights_bf = (raised / lax.optimization_barrier(jnp.sum(raised, axis=-1, keepdims=True))).astype(jnp.bfloat16)
    return jnp.einsum('hqk,khe->qhe', weights_bf.astype(jnp.float32), values_all.astype(jnp.float32)).astype(jnp.bfloat16)

def reference(tokens, documents, norm_gain, w_query, w_key, w_value, w_out, rel_bias):
    reach_rows = LEFT * SEG
    block_count = TOKENS // TOK_DEV
    current = tokens
    doc_pad = jnp.concatenate([jnp.zeros((reach_rows,), jnp.int32), documents.astype(jnp.int32)])
    for depth_index in range(LAYERS):
        widened = current.astype(jnp.float32)
        normed = (widened * lax.rsqrt(lax.optimization_barrier(jnp.mean(widened * widened, axis=-1, keepdims=True)) + EPS) * norm_gain[depth_index]).astype(jnp.bfloat16)
        queries = jnp.dot(normed, w_query[depth_index], preferred_element_type=jnp.float32).astype(jnp.bfloat16).reshape(TOKENS, HEADS, HEAD_DIM)
        keys_all = jnp.dot(normed, w_key[depth_index], preferred_element_type=jnp.float32).astype(jnp.bfloat16).reshape(TOKENS, HEADS, HEAD_DIM)
        values_all = jnp.dot(normed, w_value[depth_index], preferred_element_type=jnp.float32).astype(jnp.bfloat16).reshape(TOKENS, HEADS, HEAD_DIM)
        zero_rows = jnp.zeros((reach_rows, HEADS, HEAD_DIM), jnp.bfloat16)
        key_pad = jnp.concatenate([zero_rows, keys_all], axis=0)
        value_pad = jnp.concatenate([zero_rows, values_all], axis=0)
        bias_table = rel_bias[depth_index]

        def one_block(block_index):
            first_row = (block_index * TOK_DEV).astype(jnp.int32)
            query_block = lax.dynamic_slice_in_dim(queries, first_row, TOK_DEV, 0)
            key_block = lax.dynamic_slice_in_dim(key_pad, first_row, reach_rows + TOK_DEV, 0)
            value_block = lax.dynamic_slice_in_dim(value_pad, first_row, reach_rows + TOK_DEV, 0)
            query_doc = lax.dynamic_slice_in_dim(documents, first_row, TOK_DEV, 0)
            key_doc = lax.dynamic_slice_in_dim(doc_pad, first_row, reach_rows + TOK_DEV, 0)
            query_pos = first_row + jnp.arange(TOK_DEV, dtype=jnp.int32)
            key_pos = first_row - reach_rows + jnp.arange(reach_rows + TOK_DEV, dtype=jnp.int32)
            return attend(query_block, key_block, value_block, query_pos, key_pos, query_doc, key_doc, bias_table)
        attended = lax.map(one_block, jnp.arange(block_count, dtype=jnp.int32)).reshape(TOKENS, HEADS * HEAD_DIM)
        product = jnp.dot(attended, w_out[depth_index], preferred_element_type=jnp.float32)
        current = (widened + product).astype(jnp.bfloat16)
    return current
```

```python
import jax
import jax.numpy as jnp
from jax import lax
from jax.experimental import pallas as pl
from jax.experimental.pallas import tpu as pltpu
from jax.sharding import Mesh
from jax.sharding import PartitionSpec as P

HEAD_DIM = 64
SEG = 64
LEFT = 4
REL_CLIP = 128
EPS = 1e-06
REACH = LEFT * SEG
Q_BLOCK = 2 * SEG
K_BLOCK = Q_BLOCK + REACH
SP = ("z", "x", "c")
NEG = -1e30


def to_all(x, axis):
    length = lax.axis_size(axis)
    return lax.all_to_all(jnp.broadcast_to(x[None], (length, *x.shape)), axis, 0, 0, tiled=True)


def spread(x):
    over_z = to_all(x, "z")
    return to_all(over_z, "x")


def lay(w_ref, into):
    n_x, n_z, rows = w_ref.shape[:3]
    for z in range(n_z):
        for x in range(n_x):
            at = (z * n_x + x) * rows
            into[at : at + rows, :] = w_ref[x, z]


def query_key_kernel(halo, own, w_qk, q_out, k_out, w_all):
    lay(w_qk, w_all)
    width = q_out.shape[1]
    rows = halo.shape[0]
    before = jnp.dot(halo[...], w_all[:, width:], preferred_element_type=jnp.float32)
    k_out[:rows, :] = before.astype(jnp.bfloat16)
    for i in range(own.shape[0]):
        both = jnp.dot(own[i], w_all[...], preferred_element_type=jnp.float32).astype(jnp.bfloat16)
        q_out[i * rows : (i + 1) * rows, :] = both[:, :width]
        k_out[(i + 1) * rows : (i + 2) * rows, :] = both[:, width:]


def attend_kernel(halo, own, w_v, q, k, line, q_doc, k_doc, out, w_all, v):
    lay(w_v, w_all)
    rows = halo.shape[0]
    v[:rows, :] = jnp.dot(halo[...], w_all[...], preferred_element_type=jnp.float32).astype(jnp.bfloat16)
    for i in range(own.shape[0]):
        v[(i + 1) * rows : (i + 2) * rows, :] = jnp.dot(
            own[i], w_all[...], preferred_element_type=jnp.float32
        ).astype(jnp.bfloat16)
    q_seg = lax.broadcasted_iota(jnp.int32, (Q_BLOCK, K_BLOCK), 0) // SEG
    k_seg = lax.broadcasted_iota(jnp.int32, (Q_BLOCK, K_BLOCK), 1) // SEG
    window = (k_seg >= q_seg) & (k_seg <= q_seg + LEFT)
    blocks = q.shape[0] // Q_BLOCK
    same = []
    for b in range(blocks):
        lo = b * Q_BLOCK
        same.append((q_doc[lo : lo + Q_BLOCK, :] == k_doc[:, lo : lo + K_BLOCK]) & window)
    for h in range(q.shape[1] // HEAD_DIM):
        cols = slice(h * HEAD_DIM, (h + 1) * HEAD_DIM)
        flat = jnp.broadcast_to(line[h : h + 1, :], (Q_BLOCK, line.shape[1]))
        bias = pltpu.roll(flat, 0, 1, stride=1, stride_axis=0)[:, :K_BLOCK]
        for b in range(blocks):
            lo = b * Q_BLOCK
            scores = lax.dot_general(
                q[lo : lo + Q_BLOCK, cols],
                k[lo : lo + K_BLOCK, cols],
                (((1,), (1,)), ((), ())),
                preferred_element_type=jnp.float32,
            )
            scores = jnp.where(same[b], scores * HEAD_DIM ** (-0.5) + bias, NEG)
            peak = jnp.max(scores, axis=1, keepdims=True)
            raised = jnp.exp(scores - peak)
            total = jnp.sum(raised, axis=1, keepdims=True)
            weights = (raised / total).astype(jnp.bfloat16)
            mixed = jnp.dot(weights, v[lo : lo + K_BLOCK, cols], preferred_element_type=jnp.float32)
            out[lo : lo + Q_BLOCK, cols] = mixed.astype(jnp.bfloat16)


def project_kernel(att, w_o, out):
    n_x, n_z, rows, width = w_o.shape[1:]
    lanes = n_x * rows
    for z in range(n_z):
        total = None
        for c in range(att.shape[0]):
            part = lax.dot_general(
                att[c],
                w_o[c, :, z].reshape(lanes, width),
                (((1,), (1,)), ((), ())),
                preferred_element_type=jnp.float32,
            )
            total = part if total is None else total + part
        out[:, z * lanes : (z + 1) * lanes] = total.astype(jnp.bfloat16)


def in_vmem(kernel, outs, scratch=(), flops=10**9):
    one = not isinstance(outs, (list, tuple))
    shapes = [outs] if one else list(outs)
    specs = [pl.BlockSpec(memory_space=pltpu.VMEM) for _ in shapes]

    def call(*args):
        return pl.pallas_call(
            kernel,
            out_shape=shapes[0] if one else shapes,
            in_specs=[pl.BlockSpec(memory_space=pltpu.VMEM) for _ in args],
            out_specs=specs[0] if one else specs,
            scratch_shapes=list(scratch),
            cost_estimate=pl.CostEstimate(flops=flops, bytes_accessed=4 * 2**20, transcendentals=0),
        )(*args)

    return call


def bias_line(table):
    far = table[:, 2 * REL_CLIP :]
    near = table[:, 1:][:, ::-1]
    heads = table.shape[0]
    return jnp.concatenate(
        [
            jnp.broadcast_to(far, (heads, REACH - REL_CLIP)),
            near,
            table[:, :1],
            jnp.broadcast_to(far, (heads, Q_BLOCK - 1)),
        ],
        axis=1,
    )


def body(tokens, documents, norm_gain, w_query, w_key, w_value, w_out, rel_bias):
    rows, width = tokens.shape
    local = w_query.shape[2]
    half = local // 2
    core = lax.axis_index("c")
    tp = lax.axis_index("tp")
    n_tp = lax.axis_size("tp")
    chip = lax.axis_index("z") * lax.axis_size("x") + lax.axis_index("x")
    chips = lax.axis_size("z") * lax.axis_size("x")

    piece = w_query.shape[1]
    w_mine = lax.dynamic_slice_in_dim(w_out[0].T, tp * local, local, 1)
    packed = jnp.stack(
        [
            jnp.concatenate([w[:, c * half : (c + 1) * half] for w in (w_query[0], w_key[0], w_value[0], w_mine)], axis=1)
            for c in range(2)
        ]
    )
    mine = lax.all_to_all(packed, "c", 0, 0, tiled=True).reshape(2 * piece, 4 * half)
    w_qk = spread(mine[:, : 2 * half])
    w_v = spread(mine[:, 2 * half : 3 * half])
    w_o = to_all(spread(mine[:, 3 * half :]), "c")

    widened = tokens.astype(jnp.float32)
    normed = (
        widened * lax.rsqrt(jnp.mean(widened * widened, axis=-1, keepdims=True) + EPS) * norm_gain[0]
    ).astype(jnp.bfloat16)
    own = to_all(normed, "c")
    docs = to_all(documents, "c")
    onward = [(2 * i + c, 2 * i + 2 + c) for i in range(chips - 1) for c in range(2)]
    part = rows // 2
    sent = lax.dynamic_slice_in_dim(own[1], core * part, part, 0)
    halo, prior = lax.ppermute((sent, docs[1]), SP, onward)
    halo = to_all(halo, "c").reshape(rows, width)
    prior = jnp.where(chip > 0, prior, -1)
    docs = docs.reshape(-1)
    k_doc = jnp.concatenate([prior, docs])[None, :]
    q_doc = docs[:, None]
    line = bias_line(lax.dynamic_slice_in_dim(rel_bias[0], core * (rel_bias.shape[1] // 2), rel_bias.shape[1] // 2, 0))

    bf = jnp.bfloat16
    q, k = in_vmem(
        query_key_kernel,
        [jax.ShapeDtypeStruct((2 * rows, half), bf), jax.ShapeDtypeStruct((3 * rows, half), bf)],
        [pltpu.VMEM((width, 2 * half), bf)],
    )(halo, own, w_qk)
    att = in_vmem(
        attend_kernel,
        jax.ShapeDtypeStruct((2 * rows, half), bf),
        [pltpu.VMEM((width, half), bf), pltpu.VMEM((3 * rows, half), bf)],
    )(halo, own, w_v, q, k, line, q_doc, k_doc)
    att = lax.all_to_all(att.reshape(2, rows, half), "c", 0, 0, tiled=True)
    partial = in_vmem(project_kernel, jax.ShapeDtypeStruct((rows, width), bf))(att, w_o)
    share = rows // n_tp
    partial = lax.all_to_all(partial.reshape(n_tp, share, width), "tp", 0, 0, tiled=True)
    at = lax.dynamic_slice_in_dim(tokens, tp * share, share, 0).astype(jnp.float32)
    mixed = (at + jnp.sum(partial.astype(jnp.float32), axis=0)).astype(bf)
    return to_all(mixed, "tp").reshape(rows, width)


def solution(mesh):
    split = Mesh(mesh.devices.reshape(16, 4, 2, mesh.shape["tp"]), ("z", "x", "c", "tp"))
    placed = (
        P(SP, None),
        P(SP),
        P(),
        P(None, SP, "tp"),
        P(None, SP, "tp"),
        P(None, SP, "tp"),
        P(None, None, SP),
        P(None, "tp", None),
    )
    return jax.shard_map(body, mesh=split, in_specs=placed, out_specs=P(SP, None), check_vma=False)
```

```python
import jax
import jax.numpy as jnp
from jax import lax
from jax.experimental import pallas as pl
from jax.experimental.pallas import tpu as pltpu
from jax.sharding import Mesh
from jax.sharding import PartitionSpec as P

HEAD_DIM = 64
SEG = 64
LEFT = 4
REL_CLIP = 128
EPS = 1e-06
REACH = LEFT * SEG
Q_BLOCK = 2 * SEG
K_BLOCK = Q_BLOCK + REACH
SP = ("zh", "zl", "x", "c")
NEG = -1e30


def to_all(x, axis):
    length = lax.axis_size(axis)
    return lax.all_to_all(jnp.broadcast_to(x[None], (length, *x.shape)), axis, 0, 0, tiled=True)


def lay(w_ref, cols, into):
    n_x, n_l, n_h, rows = w_ref.shape[:4]
    for h in range(n_h):
        for l in range(n_l):
            for x in range(n_x):
                at = ((h * n_l + l) * n_x + x) * rows
                into[at : at + rows, :] = w_ref[x, l, h, :, cols]


def query_key_kernel(halo, first, second, w_in, q_out, k_out, w_all):
    width = q_out.shape[1]
    rows = halo.shape[0]
    lay(w_in, slice(0, 2 * width), w_all)
    before = jnp.dot(halo[...], w_all[:, width:], preferred_element_type=jnp.float32)
    k_out[:rows, :] = before.astype(jnp.bfloat16)
    for i, own in enumerate((first, second)):
        both = jnp.dot(own[...], w_all[...], preferred_element_type=jnp.float32).astype(jnp.bfloat16)
        q_out[i * rows : (i + 1) * rows, :] = both[:, :width]
        k_out[(i + 1) * rows : (i + 2) * rows, :] = both[:, width:]


def attend_kernel(halo, first, second, w_in, q, k, line, q_doc, k_doc, out, w_all, v):
    width = q.shape[1]
    rows = halo.shape[0]
    lay(w_in, slice(2 * width, 3 * width), w_all)
    for i, part in enumerate((halo, first, second)):
        v[i * rows : (i + 1) * rows, :] = jnp.dot(
            part[...], w_all[...], preferred_element_type=jnp.float32
        ).astype(jnp.bfloat16)
    q_seg = lax.broadcasted_iota(jnp.int32, (Q_BLOCK, K_BLOCK), 0) // SEG
    k_seg = lax.broadcasted_iota(jnp.int32, (Q_BLOCK, K_BLOCK), 1) // SEG
    window = (k_seg >= q_seg) & (k_seg <= q_seg + LEFT)
    blocks = q.shape[0] // Q_BLOCK
    same = []
    for b in range(blocks):
        lo = b * Q_BLOCK
        same.append((q_doc[lo : lo + Q_BLOCK, :] == k_doc[:, lo : lo + K_BLOCK]) & window)
    for h in range(q.shape[1] // HEAD_DIM):
        cols = slice(h * HEAD_DIM, (h + 1) * HEAD_DIM)
        flat = jnp.broadcast_to(line[h : h + 1, :], (Q_BLOCK, line.shape[1]))
        bias = pltpu.roll(flat, 0, 1, stride=1, stride_axis=0)[:, :K_BLOCK]
        for b in range(blocks):
            lo = b * Q_BLOCK
            scores = lax.dot_general(
                q[lo : lo + Q_BLOCK, cols],
                k[lo : lo + K_BLOCK, cols],
                (((1,), (1,)), ((), ())),
                preferred_element_type=jnp.float32,
            )
            scores = jnp.where(same[b], scores * HEAD_DIM ** (-0.5) + bias, NEG)
            peak = jnp.max(scores, axis=1, keepdims=True)
            raised = jnp.exp(scores - peak)
            total = jnp.sum(raised, axis=1, keepdims=True)
            mixed = jnp.dot(
                raised.astype(jnp.bfloat16), v[lo : lo + K_BLOCK, cols], preferred_element_type=jnp.float32
            )
            out[lo : lo + Q_BLOCK, cols] = (mixed / total).astype(jnp.bfloat16)


def project_kernel(att, w_o, out):
    n_x, n_l, n_h, rows, width = w_o.shape[1:]
    lanes = n_x * rows
    for h in range(n_h):
        for l in range(n_l):
            total = None
            for c in range(att.shape[0]):
                part = lax.dot_general(
                    att[c],
                    w_o[c, :, l, h].reshape(lanes, width),
                    (((1,), (1,)), ((), ())),
                    preferred_element_type=jnp.float32,
                )
                total = part if total is None else total + part
            at = (h * n_l + l) * lanes
            out[:, at : at + lanes] = total.astype(jnp.bfloat16)


def in_vmem(kernel, outs, scratch=(), grant=16, flops=2 * 10**10):
    one = not isinstance(outs, (list, tuple))
    shapes = [outs] if one else list(outs)
    specs = [pl.BlockSpec(memory_space=pltpu.VMEM) for _ in shapes]

    def call(*args):
        return pl.pallas_call(
            kernel,
            out_shape=shapes[0] if one else shapes,
            in_specs=[pl.BlockSpec(memory_space=pltpu.VMEM) for _ in args],
            out_specs=specs[0] if one else specs,
            scratch_shapes=list(scratch),
            compiler_params=pltpu.CompilerParams(vmem_limit_bytes=grant * 2**20),
            cost_estimate=pl.CostEstimate(flops=flops, bytes_accessed=4 * 2**20, transcendentals=0),
        )(*args)

    return call


def bias_line(table):
    far = table[:, 2 * REL_CLIP :]
    near = table[:, 1:][:, ::-1]
    heads = table.shape[0]
    return jnp.concatenate(
        [
            jnp.broadcast_to(far, (heads, REACH - REL_CLIP)),
            near,
            table[:, :1],
            jnp.broadcast_to(far, (heads, Q_BLOCK - 1)),
        ],
        axis=1,
    )


def body(tokens, documents, norm_gain, w_query, w_key, w_value, w_out, rel_bias):
    rows, width = tokens.shape
    local = w_query.shape[2]
    half = local // 2
    core = lax.axis_index("c")
    tp = lax.axis_index("tp")
    n_tp = lax.axis_size("tp")
    chips = lax.axis_size(SP[:-1])
    chip = lax.axis_index(SP[:-1])

    piece = w_query.shape[1]
    w_mine = lax.dynamic_slice_in_dim(w_out[0].T, tp * local, local, 1)
    packed = jnp.stack(
        [
            jnp.concatenate([w[:, c * half : (c + 1) * half] for w in (w_query[0], w_key[0], w_value[0], w_mine)], axis=1)
            for c in range(2)
        ]
    )
    mine = lax.all_to_all(packed, "c", 0, 0, tiled=True).reshape(2 * piece, 4 * half)
    over_z = to_all(to_all(mine, "zh"), "zl")
    w_in = to_all(over_z[..., : 3 * half], "x")
    last, w_in = lax.optimization_barrier((over_z[..., 3 * half :], w_in))
    last = to_all(last, "x")

    widened = tokens.astype(jnp.float32)
    normed = (
        widened * lax.rsqrt(jnp.mean(widened * widened, axis=-1, keepdims=True) + EPS) * norm_gain[0]
    ).astype(jnp.bfloat16)
    swap = [(0, 1), (1, 0)]
    other, other_doc = lax.ppermute((normed, documents), "c", swap)
    first, second = jnp.where(core == 0, normed, other), jnp.where(core == 0, other, normed)
    doc_1, doc_2 = jnp.where(core == 0, documents, other_doc), jnp.where(core == 0, other_doc, documents)
    onward = [(2 * i + c, 2 * i + 2 + c) for i in range(chips - 1) for c in range(2)]
    halo, prior = lax.ppermute((second, doc_2), SP, onward)
    prior = jnp.where(chip > 0, prior, -1)
    k_doc = jnp.concatenate([prior, doc_1, doc_2])[None, :]
    q_doc = jnp.concatenate([doc_1, doc_2])[:, None]
    line = bias_line(lax.dynamic_slice_in_dim(rel_bias[0], core * (rel_bias.shape[1] // 2), rel_bias.shape[1] // 2, 0))

    bf = jnp.bfloat16
    q, k = in_vmem(
        query_key_kernel,
        [jax.ShapeDtypeStruct((2 * rows, half), bf), jax.ShapeDtypeStruct((3 * rows, half), bf)],
        [pltpu.VMEM((width, 2 * half), bf)],
    )(halo, first, second, w_in)
    q, k, last = lax.optimization_barrier((q, k, last))
    w_o = to_all(last, "c")
    att = in_vmem(
        attend_kernel,
        jax.ShapeDtypeStruct((2 * rows, half), bf),
        [pltpu.VMEM((width, half), bf), pltpu.VMEM((3 * rows, half), bf)],
    )(halo, first, second, w_in, q, k, line, q_doc, k_doc)
    att, w_o = lax.optimization_barrier((att, w_o))
    att = lax.all_to_all(att.reshape(2, rows, half), "c", 0, 0, tiled=True)
    partial = in_vmem(project_kernel, jax.ShapeDtypeStruct((rows, width), bf))(att, w_o)
    share = rows // n_tp
    partial = lax.all_to_all(partial.reshape(n_tp, share, width), "tp", 0, 0, tiled=True)
    at = lax.dynamic_slice_in_dim(tokens, tp * share, share, 0).astype(jnp.float32)
    mixed = (at + jnp.sum(partial.astype(jnp.float32), axis=0)).astype(bf)
    return to_all(mixed, "tp").reshape(rows, width)


def solution(mesh):
    split = Mesh(mesh.devices.reshape(4, 4, 4, 2, mesh.shape["tp"]), (*SP, "tp"))
    placed = (
        P(SP, None),
        P(SP),
        P(),
        P(None, SP, "tp"),
        P(None, SP, "tp"),
        P(None, SP, "tp"),
        P(None, None, SP),
        P(None, "tp", None),
    )
    return jax.shard_map(body, mesh=split, in_specs=placed, out_specs=P(SP, None), check_vma=False)
```

```python
import jax
import jax.numpy as jnp
from jax import lax
from jax.experimental import pallas as pl
from jax.experimental.pallas import tpu as pltpu
from jax.sharding import Mesh
from jax.sharding import PartitionSpec as P

HEAD_DIM = 64
SEG = 64
LEFT = 4
REL_CLIP = 128
EPS = 1e-06
REACH = LEFT * SEG
Q_BLOCK = 2 * SEG
K_BLOCK = Q_BLOCK + REACH
SP = ("zh", "zl", "x", "c")
NEG = -1e30


def to_all(x, axis):
    length = lax.axis_size(axis)
    return lax.all_to_all(jnp.broadcast_to(x[None], (length, *x.shape)), axis, 0, 0, tiled=True)


def lay(w_ref, cols, into):
    n_x, n_l, n_h, rows = w_ref.shape[:4]
    for h in range(n_h):
        for l in range(n_l):
            for x in range(n_x):
                at = ((h * n_l + l) * n_x + x) * rows
                into[at : at + rows, :] = w_ref[x, l, h, :, cols]


def norm_kernel(tokens, gain, docs, out):
    rows = tokens.shape[0]
    wide = tokens[...].astype(jnp.float32)
    scale = lax.rsqrt(jnp.mean(wide * wide, axis=1, keepdims=True) + EPS)
    out[:rows, :] = (wide * scale * gain[...]).astype(jnp.bfloat16)
    extra = out.shape[0] - rows
    out[rows:, :rows] = jnp.broadcast_to(docs[...].astype(jnp.float32), (extra, rows)).astype(jnp.bfloat16)
    out[rows:, rows:] = jnp.zeros((extra, out.shape[1] - rows), jnp.bfloat16)


def attend_kernel(ids, halo, mine, other, w_in, line, out, w_all, q, k, v, docs):
    width = q.shape[1]
    rows = q.shape[0] // 2
    core = ids[0]
    lay(w_in, slice(0, 3 * width), w_all)

    def doc_row(part):
        return part[rows : rows + 16, :rows].astype(jnp.float32)[0:1]

    docs[0:1, :rows] = jnp.where(ids[1] > 0, doc_row(halo), -1.0)
    before = jnp.dot(halo[:rows, :], w_all[:, width:], preferred_element_type=jnp.float32).astype(jnp.bfloat16)
    k[:rows, :] = before[:, :width]
    v[:rows, :] = before[:, width:]
    for part, at in ((mine, core), (other, 1 - core)):
        total = jnp.dot(part[:rows, :], w_all[...], preferred_element_type=jnp.float32).astype(jnp.bfloat16)
        to = pl.multiple_of(at * rows, rows)
        q[pl.ds(to, rows), :] = total[:, :width]
        k[pl.ds(to + rows, rows), :] = total[:, width : 2 * width]
        v[pl.ds(to + rows, rows), :] = total[:, 2 * width :]
    docs[0:1, rows : 2 * rows] = jnp.where(core == 0, doc_row(mine), doc_row(other))
    docs[0:1, 2 * rows :] = jnp.where(core == 0, doc_row(other), doc_row(mine))
    q_seg = lax.broadcasted_iota(jnp.int32, (Q_BLOCK, K_BLOCK), 0) // SEG
    k_seg = lax.broadcasted_iota(jnp.int32, (Q_BLOCK, K_BLOCK), 1) // SEG
    window = (k_seg >= q_seg) & (k_seg <= q_seg + LEFT)
    blocks = q.shape[0] // Q_BLOCK
    same = []
    for b in range(blocks):
        lo = b * Q_BLOCK
        across = jnp.broadcast_to(docs[0:1, rows + lo : rows + lo + Q_BLOCK], (Q_BLOCK, Q_BLOCK))
        down = jnp.concatenate([across.T] * (K_BLOCK // Q_BLOCK), axis=1)
        same.append((down == docs[0:1, lo : lo + K_BLOCK]) & window)
    for h in range(q.shape[1] // HEAD_DIM):
        cols = slice(h * HEAD_DIM, (h + 1) * HEAD_DIM)
        flat = jnp.broadcast_to(line[h : h + 1, :], (Q_BLOCK, line.shape[1]))
        bias = pltpu.roll(flat, 0, 1, stride=1, stride_axis=0)[:, :K_BLOCK]
        for b in range(blocks):
            lo = b * Q_BLOCK
            scores = lax.dot_general(
                q[lo : lo + Q_BLOCK, cols],
                k[lo : lo + K_BLOCK, cols],
                (((1,), (1,)), ((), ())),
                preferred_element_type=jnp.float32,
            )
            scores = jnp.where(same[b], scores * HEAD_DIM ** (-0.5) + bias, NEG)
            peak = jnp.max(scores, axis=1, keepdims=True)
            raised = jnp.exp(scores - peak)
            total = jnp.sum(raised, axis=1, keepdims=True)
            mixed = jnp.dot(
                raised.astype(jnp.bfloat16), v[lo : lo + K_BLOCK, cols], preferred_element_type=jnp.float32
            )
            out[lo : lo + Q_BLOCK, cols] = (mixed / total).astype(jnp.bfloat16)


def project_kernel(ids, att, w_in, w_other, out):
    n_x, n_l, n_h, rows, width = w_other.shape
    lanes = n_x * rows
    core = ids[0]
    start = w_in.shape[-1] - width
    for h in range(n_h):
        for l in range(n_l):
            mine = w_in[:, l, h, :, start:].reshape(lanes, width)
            other = w_other[:, l, h].reshape(lanes, width)
            total = sum(
                lax.dot_general(att[i], w, (((1,), (1,)), ((), ())), preferred_element_type=jnp.float32)
                for i, w in ((core, mine), (1 - core, other))
            )
            at = (h * n_l + l) * lanes
            out[:, at : at + lanes] = total.astype(jnp.bfloat16)


def in_vmem(kernel, outs, scratch=(), grant=16, flops=2 * 10**10):
    one = not isinstance(outs, (list, tuple))
    shapes = [outs] if one else list(outs)
    specs = [pl.BlockSpec(memory_space=pltpu.VMEM) for _ in shapes]

    def call(*args):
        return pl.pallas_call(
            kernel,
            out_shape=shapes[0] if one else shapes,
            in_specs=[pl.BlockSpec(memory_space=pltpu.SMEM if a.shape == (2,) else pltpu.VMEM) for a in args],
            out_specs=specs[0] if one else specs,
            scratch_shapes=list(scratch),
            compiler_params=pltpu.CompilerParams(vmem_limit_bytes=grant * 2**20),
            cost_estimate=pl.CostEstimate(flops=flops, bytes_accessed=4 * 2**20, transcendentals=0),
        )(*args)

    return call


def bias_line(table):
    far = table[:, 2 * REL_CLIP :]
    near = table[:, 1:][:, ::-1]
    heads = table.shape[0]
    return jnp.concatenate(
        [
            jnp.broadcast_to(far, (heads, REACH - REL_CLIP)),
            near,
            table[:, :1],
            jnp.broadcast_to(far, (heads, Q_BLOCK - 1)),
        ],
        axis=1,
    )


def body(tokens, documents, norm_gain, w_query, w_key, w_value, w_out, rel_bias):
    rows, width = tokens.shape
    local = w_query.shape[2]
    half = local // 2
    core = lax.axis_index("c")
    tp = lax.axis_index("tp")
    n_tp = lax.axis_size("tp")
    chips = lax.axis_size(SP[:-1])
    chip = lax.axis_index(SP[:-1])

    piece = w_query.shape[1]
    w_mine = lax.dynamic_slice_in_dim(w_out[0].T, tp * local, local, 1)
    packed = jnp.stack(
        [
            jnp.concatenate([w[:, c * half : (c + 1) * half] for w in (w_query[0], w_key[0], w_value[0], w_mine)], axis=1)
            for c in range(2)
        ]
    )
    bf = jnp.bfloat16
    share = rows // n_tp
    at = lax.dynamic_slice_in_dim(tokens, tp * share, share, 0).astype(jnp.float32)
    line = bias_line(lax.dynamic_slice_in_dim(rel_bias[0], core * (rel_bias.shape[1] // 2), rel_bias.shape[1] // 2, 0))
    ids = jnp.stack([core, chip])
    block = in_vmem(norm_kernel, jax.ShapeDtypeStruct((rows + 16, width), bf), flops=10**9)(
        tokens, norm_gain, documents[None, :]
    )
    other = lax.ppermute(block, "c", [(0, 1), (1, 0)])
    mine = lax.all_to_all(packed, "c", 0, 0, tiled=True).reshape(2 * piece, 4 * half)
    last = jnp.where(core == 0, other, block)
    last, mine, line, at, ids = lax.optimization_barrier((last, mine, line, at, ids))
    onward = [(2 * i + c, 2 * i + 2 + c) for i in range(chips - 1) for c in range(2)]
    halo = lax.ppermute(last, SP, onward)
    over_far = to_all(mine, "zh")
    w_in = to_all(to_all(over_far, "zl"), "x")
    w_other = lax.ppermute(w_in[..., 3 * half :], "c", [(0, 1), (1, 0)])
    att = in_vmem(
        attend_kernel,
        jax.ShapeDtypeStruct((2 * rows, half), bf),
        [
            pltpu.VMEM((width, 3 * half), bf),
            pltpu.VMEM((2 * rows, half), bf),
            pltpu.VMEM((3 * rows, half), bf),
            pltpu.VMEM((3 * rows, half), bf),
            pltpu.VMEM((8, 3 * rows), jnp.float32),
        ],
    )(ids, halo, block, other, w_in, line)
    att = lax.all_to_all(att.reshape(2, rows, half), "c", 0, 0, tiled=True)
    partial = in_vmem(project_kernel, jax.ShapeDtypeStruct((rows, width), bf))(ids, att, w_in, w_other)
    partial = lax.all_to_all(partial.reshape(n_tp, share, width), "tp", 0, 0, tiled=True)
    mixed = (at + jnp.sum(partial.astype(jnp.float32), axis=0)).astype(bf)
    return to_all(mixed, "tp").reshape(rows, width)


def solution(mesh):
    split = Mesh(mesh.devices.reshape(4, 4, 4, 2, mesh.shape["tp"]), (*SP, "tp"))
    placed = (
        P(SP, None),
        P(SP),
        P(),
        P(None, SP, "tp"),
        P(None, SP, "tp"),
        P(None, SP, "tp"),
        P(None, None, SP),
        P(None, "tp", None),
    )

    def step(*args):
        return body(*args)

    step = jax.shard_map(step, mesh=split, in_specs=placed, out_specs=P(SP, None), check_vma=False)
    return step
```

```python
import jax
import jax.numpy as jnp
from jax import lax
from jax.experimental import pallas as pl
from jax.experimental.pallas import tpu as pltpu
from jax.sharding import Mesh
from jax.sharding import PartitionSpec as P

HEAD_DIM = 64
SEG = 64
LEFT = 4
REL_CLIP = 128
EPS = 1e-06
REACH = LEFT * SEG
Q_BLOCK = 2 * SEG
K_BLOCK = Q_BLOCK + REACH
SP = ("zh", "zl", "x", "c")
NEG = -1e30


def to_all(x, axis):
    length = lax.axis_size(axis)
    return lax.all_to_all(jnp.broadcast_to(x[None], (length, *x.shape)), axis, 0, 0, tiled=True)


def norm_kernel(tokens, gain, docs, out):
    rows = tokens.shape[0]
    wide = tokens[...].astype(jnp.float32)
    scale = lax.rsqrt(jnp.mean(wide * wide, axis=1, keepdims=True) + EPS)
    out[:rows, :] = (wide * scale * gain[...]).astype(jnp.bfloat16)
    extra = out.shape[0] - rows
    out[rows:, :rows] = jnp.broadcast_to(docs[...].astype(jnp.float32), (extra, rows)).astype(jnp.bfloat16)
    out[rows:, rows:] = jnp.zeros((extra, out.shape[1] - rows), jnp.bfloat16)


def qkv_kernel(ids, b0, s0, b1, s1, b2, s2, b3, s3, w_in, qkv, docs, tail, w_all):
    rows = qkv.shape[0] // 8
    n_l, n_h, lanes = w_in.shape[:3]
    for h in range(n_h):
        for l in range(n_l):
            at = (h * n_l + l) * lanes
            w_all[at : at + lanes, :] = w_in[l, h]
    core, x = ids[0], ids[1]
    for back, pair in enumerate(((b0, s0), (b1, s1), (b2, s2), (b3, s3))):
        for c, part in zip((core, 1 - core), pair):
            at = ((x + 4 - back) & 3) * 2 + c
            total = jnp.dot(part[:rows, :], w_all[...], preferred_element_type=jnp.float32)
            qkv[pl.ds(pl.multiple_of(at * rows, rows), rows), :] = total.astype(jnp.bfloat16)
            docs[pl.ds(at, 1), :] = part[rows : rows + 16, :rows].astype(jnp.float32)[0:1]
    tail[:rows, :] = qkv[7 * rows :, :]
    tail[rows:, :] = jnp.broadcast_to(docs[7:8, :], (16, rows)).astype(jnp.bfloat16)


def attend_kernel(ids, qkv, halo, docs, line, out):
    rows = docs.shape[1]
    flat = jnp.broadcast_to(line[...], (Q_BLOCK, line.shape[1]))
    bias = pltpu.roll(flat, 0, 1, stride=1, stride_axis=0)[:, :K_BLOCK]
    q_seg = lax.broadcasted_iota(jnp.int32, (Q_BLOCK, K_BLOCK), 0) // SEG
    k_seg = lax.broadcasted_iota(jnp.int32, (Q_BLOCK, K_BLOCK), 1) // SEG
    bias = jnp.where((k_seg >= q_seg) & (k_seg <= q_seg + LEFT), bias, NEG)
    prior = jnp.where(ids[2] > 0, halo[rows : rows + 16, :].astype(jnp.float32)[0:1], -1.0)

    def doc_part(b):
        if b < 0:
            return prior[:, rows + b * Q_BLOCK : rows + (b + 1) * Q_BLOCK]
        at = b * Q_BLOCK % rows
        return docs[b * Q_BLOCK // rows : b * Q_BLOCK // rows + 1, at : at + Q_BLOCK]

    def row_part(b, cols):
        if b < 0:
            return halo[rows + b * Q_BLOCK : rows + (b + 1) * Q_BLOCK, cols]
        return qkv[b * Q_BLOCK : (b + 1) * Q_BLOCK, cols]

    def key_rows(b, cols):
        if b >= 2:
            return qkv[(b - 2) * Q_BLOCK : (b + 1) * Q_BLOCK, cols]
        return jnp.concatenate([row_part(i, cols) for i in range(b - 2, b + 1)], axis=0)

    for b in range(qkv.shape[0] // Q_BLOCK):
        across = jnp.broadcast_to(doc_part(b), (Q_BLOCK, Q_BLOCK)).T
        same = jnp.concatenate([across == doc_part(i) for i in range(b - 2, b + 1)], axis=1)
        scores = lax.dot_general(
            qkv[b * Q_BLOCK : (b + 1) * Q_BLOCK, :HEAD_DIM],
            key_rows(b, slice(HEAD_DIM, 2 * HEAD_DIM)),
            (((1,), (1,)), ((), ())),
            preferred_element_type=jnp.float32,
        )
        scores = jnp.where(same, scores * HEAD_DIM ** (-0.5) + bias, NEG)
        peak = jnp.max(scores, axis=1, keepdims=True)
        raised = jnp.exp(scores - peak)
        total = jnp.sum(raised, axis=1, keepdims=True)
        mixed = jnp.dot(
            raised.astype(jnp.bfloat16),
            key_rows(b, slice(2 * HEAD_DIM, 3 * HEAD_DIM)),
            preferred_element_type=jnp.float32,
        )
        lane = b % 2 * HEAD_DIM
        out[b // 2, :, lane : lane + HEAD_DIM] = (mixed / total).astype(jnp.bfloat16)


def out_rows_kernel(w_in, out):
    n_l, n_h = w_in.shape[:2]
    for h in range(n_h):
        for l in range(n_l):
            at = (h * n_l + l) * 16
            out[at : at + 16, :] = jnp.concatenate(
                [w_in[l, h, 16 * j : 16 * j + 16, 3 * HEAD_DIM :] for j in range(8)], axis=1
            )


def project_kernel(ids, att, w_mine, w_other, out, lhs, rhs):
    half = att.shape[1]
    for i in range(att.shape[0]):
        lhs[:half, i * HEAD_DIM : (i + 1) * HEAD_DIM] = att[i, :, :HEAD_DIM]
        lhs[half:, i * HEAD_DIM : (i + 1) * HEAD_DIM] = att[i, :, HEAD_DIM:]
    core = ids[0]
    for c, w in ((core, w_mine), (1 - core, w_other)):
        for z in range(16):
            for x in range(4):
                to = pl.multiple_of(z * 128 + x * 32 + c * 16, 16)
                rhs[pl.ds(to, 16), :] = w[x, z * 16 : z * 16 + 16, :]
    out[...] = lax.dot_general(
        lhs[...], rhs[...], (((1,), (1,)), ((), ())), preferred_element_type=jnp.float32
    ).astype(jnp.bfloat16)


def in_vmem(kernel, outs, scratch=(), grant=16, flops=2 * 10**10):
    one = not isinstance(outs, (list, tuple))
    shapes = [outs] if one else list(outs)
    specs = [pl.BlockSpec(memory_space=pltpu.VMEM) for _ in shapes]

    def call(*args):
        return pl.pallas_call(
            kernel,
            out_shape=shapes[0] if one else shapes,
            in_specs=[pl.BlockSpec(memory_space=pltpu.SMEM if a.ndim == 1 else pltpu.VMEM) for a in args],
            out_specs=specs[0] if one else specs,
            scratch_shapes=list(scratch),
            compiler_params=pltpu.CompilerParams(vmem_limit_bytes=grant * 2**20),
            cost_estimate=pl.CostEstimate(flops=flops, bytes_accessed=4 * 2**20, transcendentals=0),
        )(*args)

    return call


def bias_line(table):
    far = table[:, 2 * REL_CLIP :]
    near = table[:, 1:][:, ::-1]
    heads = table.shape[0]
    return jnp.concatenate(
        [
            jnp.broadcast_to(far, (heads, REACH - REL_CLIP)),
            near,
            table[:, :1],
            jnp.broadcast_to(far, (heads, Q_BLOCK - 1)),
        ],
        axis=1,
    )


def body(tokens, documents, norm_gain, w_query, w_key, w_value, w_out, rel_bias):
    rows, width = tokens.shape
    local = w_query.shape[2]
    core = lax.axis_index("c")
    x = lax.axis_index("x")
    z = lax.axis_index(("zh", "zl"))
    tp = lax.axis_index("tp")
    n_tp = lax.axis_size("tp")
    plane = ("x", "c")
    group = lax.axis_size(plane)
    bf = jnp.bfloat16

    piece = w_query.shape[1]
    w_mine = lax.dynamic_slice_in_dim(w_out[0].T, tp * local, local, 1)
    by_head = [w.reshape(piece, group, HEAD_DIM).swapaxes(0, 1) for w in (w_query[0], w_key[0], w_value[0], w_mine)]
    packed = jnp.concatenate(by_head[:3], axis=2)

    share = rows // n_tp
    at = lax.dynamic_slice_in_dim(tokens, tp * share, share, 0).astype(jnp.float32)
    line = bias_line(lax.dynamic_slice_in_dim(rel_bias[0], x * 2 + core, 1, 0))
    ids = jnp.stack([core, x, z])
    block = in_vmem(norm_kernel, jax.ShapeDtypeStruct((rows + 16, width), bf), flops=10**9)(
        tokens, norm_gain, documents[None, :]
    )
    swap = [(0, 1), (1, 0)]
    parts = [block, lax.ppermute(block, "c", swap)]
    mine = lax.all_to_all(packed, plane, 0, 0, tiled=True)
    mine = jnp.concatenate([mine, by_head[3]], axis=2).reshape(group * piece, 4 * HEAD_DIM)
    mine, line, at, ids = lax.optimization_barrier((mine, line, at, ids))
    for back in (1, 2, 3):
        got = lax.ppermute(block, "x", [(i, (i + back) % 4) for i in range(4)])
        parts += [got, lax.ppermute(got, "c", swap)]
    over_far = to_all(mine, "zh")
    w_in = to_all(over_far, "zl")
    rows_out = in_vmem(out_rows_kernel, jax.ShapeDtypeStruct((16 * piece, local), bf), flops=10**9)(w_in)
    w_mine = to_all(rows_out, "x")
    w_other = lax.ppermute(w_mine, "c", swap)
    qkv, docs, tail = in_vmem(
        qkv_kernel,
        [
            jax.ShapeDtypeStruct((group * rows, 4 * HEAD_DIM), bf),
            jax.ShapeDtypeStruct((group, rows), jnp.float32),
            jax.ShapeDtypeStruct((rows + 16, 4 * HEAD_DIM), bf),
        ],
        [pltpu.VMEM((width, 4 * HEAD_DIM), bf)],
        grant=24,
    )(ids, *parts, w_in)
    halo = lax.ppermute(tail, ("zh", "zl"), [(i, i + 1) for i in range(15)])
    att = in_vmem(attend_kernel, jax.ShapeDtypeStruct((group, rows // 2, 2 * HEAD_DIM), bf))(
        ids, qkv, halo, docs, line
    )
    att = lax.all_to_all(att, plane, 0, 0, tiled=True)
    partial = in_vmem(
        project_kernel,
        jax.ShapeDtypeStruct((rows, width), bf),
        [pltpu.VMEM((rows, local), bf), pltpu.VMEM((width, local), bf)],
    )(ids, att, w_mine, w_other)
    partial = lax.all_to_all(partial.reshape(n_tp, share, width), "tp", 0, 0, tiled=True)
    mixed = (at + jnp.sum(partial.astype(jnp.float32), axis=0)).astype(bf)
    return to_all(mixed, "tp").reshape(rows, width)


def solution(mesh):
    split = Mesh(mesh.devices.reshape(4, 4, 4, 2, mesh.shape["tp"]), (*SP, "tp"))
    placed = (
        P(SP, None),
        P(SP),
        P(),
        P(None, SP, "tp"),
        P(None, SP, "tp"),
        P(None, SP, "tp"),
        P(None, None, SP),
        P(None, "tp", None),
    )

    def step(*args):
        return body(*args)

    step = jax.shard_map(step, mesh=split, in_specs=placed, out_specs=P(SP, None), check_vma=False)
    return step
```

```python
import jax
import jax.numpy as jnp
from jax import lax
from jax.experimental import pallas as pl
from jax.experimental.pallas import tpu as pltpu
from jax.sharding import Mesh
from jax.sharding import PartitionSpec as P

HEAD_DIM = 64
SEG = 64
LEFT = 4
REL_CLIP = 128
EPS = 1e-06
REACH = LEFT * SEG
Q_BLOCK = 2 * SEG
K_BLOCK = Q_BLOCK + REACH
SP = ("zh", "zl", "x", "c")
NEG = -1e30


def to_all(x, axis):
    length = lax.axis_size(axis)
    return lax.all_to_all(jnp.broadcast_to(x[None], (length, *x.shape)), axis, 0, 0, tiled=True)


def pack_kernel(ids, w_q, w_k, w_v, w_o, heads, rest):
    n = heads.shape[0]
    own = w_o[:, pl.ds(pl.multiple_of(ids[3] * n * HEAD_DIM, n * HEAD_DIM), n * HEAD_DIM)]
    for i in range(n):
        cols = slice(i * HEAD_DIM, (i + 1) * HEAD_DIM)
        heads[i] = jnp.concatenate([w_q[:, cols], w_k[:, cols], w_v[:, cols]], axis=1)
        rest[i] = own[:, cols]


def sum_kernel(partial, tokens, out):
    total = tokens[...].astype(jnp.float32)
    for i in range(partial.shape[0]):
        total = total + partial[i].astype(jnp.float32)
    total = total.astype(jnp.bfloat16)
    for i in range(out.shape[0]):
        out[i] = total


def norm_kernel(tokens, gain, docs, out):
    rows = tokens.shape[0]
    wide = tokens[...].astype(jnp.float32)
    scale = lax.rsqrt(jnp.mean(wide * wide, axis=1, keepdims=True) + EPS)
    out[:rows, :] = (wide * scale * gain[...]).astype(jnp.bfloat16)
    extra = out.shape[0] - rows
    out[rows:, :rows] = jnp.broadcast_to(docs[...].astype(jnp.float32), (extra, rows)).astype(jnp.bfloat16)
    out[rows:, rows:] = jnp.zeros((extra, out.shape[1] - rows), jnp.bfloat16)


def qkv_kernel(ids, b0, s0, b1, s1, b2, s2, b3, s3, w_in, qkv, docs, tail, w_all):
    rows = qkv.shape[0] // 8
    n_l, n_h, lanes = w_in.shape[:3]
    for h in range(n_h):
        for l in range(n_l):
            at = (h * n_l + l) * lanes
            w_all[at : at + lanes, :] = w_in[l, h]
    core, x = ids[0], ids[1]
    for back, pair in enumerate(((b0, s0), (b1, s1), (b2, s2), (b3, s3))):
        for c, part in zip((core, 1 - core), pair):
            at = ((x + 4 - back) & 3) * 2 + c
            total = jnp.dot(part[:rows, :], w_all[...], preferred_element_type=jnp.float32)
            qkv[pl.ds(pl.multiple_of(at * rows, rows), rows), :] = total.astype(jnp.bfloat16)
            docs[pl.ds(at, 1), :] = part[rows : rows + 16, :rows].astype(jnp.float32)[0:1]
    tail[:rows, :] = qkv[7 * rows :, :]
    tail[rows:, :] = jnp.broadcast_to(docs[7:8, :], (16, rows)).astype(jnp.bfloat16)


def attend_kernel(ids, qkv, halo, docs, line, out):
    rows = docs.shape[1]
    flat = jnp.broadcast_to(line[...], (Q_BLOCK, line.shape[1]))
    bias = pltpu.roll(flat, 0, 1, stride=1, stride_axis=0)[:, :K_BLOCK]
    q_seg = lax.broadcasted_iota(jnp.int32, (Q_BLOCK, K_BLOCK), 0) // SEG
    k_seg = lax.broadcasted_iota(jnp.int32, (Q_BLOCK, K_BLOCK), 1) // SEG
    bias = jnp.where((k_seg >= q_seg) & (k_seg <= q_seg + LEFT), bias, NEG)
    prior = jnp.where(ids[2] > 0, halo[rows : rows + 16, :].astype(jnp.float32)[0:1], -1.0)

    def doc_part(b):
        if b < 0:
            return prior[:, rows + b * Q_BLOCK : rows + (b + 1) * Q_BLOCK]
        at = b * Q_BLOCK % rows
        return docs[b * Q_BLOCK // rows : b * Q_BLOCK // rows + 1, at : at + Q_BLOCK]

    def row_part(b, cols):
        if b < 0:
            return halo[rows + b * Q_BLOCK : rows + (b + 1) * Q_BLOCK, cols]
        return qkv[b * Q_BLOCK : (b + 1) * Q_BLOCK, cols]

    def key_rows(b, cols):
        if b >= 2:
            return qkv[(b - 2) * Q_BLOCK : (b + 1) * Q_BLOCK, cols]
        return jnp.concatenate([row_part(i, cols) for i in range(b - 2, b + 1)], axis=0)

    for b in range(qkv.shape[0] // Q_BLOCK):
        across = jnp.broadcast_to(doc_part(b), (Q_BLOCK, Q_BLOCK)).T
        same = jnp.concatenate([across == doc_part(i) for i in range(b - 2, b + 1)], axis=1)
        scores = lax.dot_general(
            qkv[b * Q_BLOCK : (b + 1) * Q_BLOCK, :HEAD_DIM],
            key_rows(b, slice(HEAD_DIM, 2 * HEAD_DIM)),
            (((1,), (1,)), ((), ())),
            preferred_element_type=jnp.float32,
        )
        scores = jnp.where(same, scores * HEAD_DIM ** (-0.5) + bias, NEG)
        peak = jnp.max(scores, axis=1, keepdims=True)
        raised = jnp.exp(scores - peak)
        total = jnp.sum(raised, axis=1, keepdims=True)
        mixed = jnp.dot(
            raised.astype(jnp.bfloat16),
            key_rows(b, slice(2 * HEAD_DIM, 3 * HEAD_DIM)),
            preferred_element_type=jnp.float32,
        )
        lane = b % 2 * HEAD_DIM
        out[b // 2, :, lane : lane + HEAD_DIM] = (mixed / total).astype(jnp.bfloat16)


def out_rows_kernel(w_in, out):
    n_l, n_h = w_in.shape[:2]
    for h in range(n_h):
        for l in range(n_l):
            at = (h * n_l + l) * 16
            out[at : at + 16, :] = jnp.concatenate(
                [w_in[l, h, 16 * j : 16 * j + 16, 3 * HEAD_DIM :] for j in range(8)], axis=1
            )


def project_kernel(ids, att, w_mine, w_other, out, lhs, rhs):
    half = att.shape[1]
    for i in range(att.shape[0]):
        lhs[:half, i * HEAD_DIM : (i + 1) * HEAD_DIM] = att[i, :, :HEAD_DIM]
        lhs[half:, i * HEAD_DIM : (i + 1) * HEAD_DIM] = att[i, :, HEAD_DIM:]
    core = ids[0]
    for c, w in ((core, w_mine), (1 - core, w_other)):
        for z in range(16):
            for x in range(4):
                to = pl.multiple_of(z * 128 + x * 32 + c * 16, 16)
                rhs[pl.ds(to, 16), :] = w[x, z * 16 : z * 16 + 16, :]
    out[...] = lax.dot_general(
        lhs[...], rhs[...], (((1,), (1,)), ((), ())), preferred_element_type=jnp.float32
    ).astype(jnp.bfloat16)


def in_vmem(kernel, outs, scratch=(), grant=16, flops=2 * 10**10):
    one = not isinstance(outs, (list, tuple))
    shapes = [outs] if one else list(outs)
    specs = [pl.BlockSpec(memory_space=pltpu.VMEM) for _ in shapes]

    def call(*args):
        return pl.pallas_call(
            kernel,
            out_shape=shapes[0] if one else shapes,
            in_specs=[pl.BlockSpec(memory_space=pltpu.SMEM if a.ndim == 1 else pltpu.VMEM) for a in args],
            out_specs=specs[0] if one else specs,
            scratch_shapes=list(scratch),
            compiler_params=pltpu.CompilerParams(vmem_limit_bytes=grant * 2**20),
            cost_estimate=pl.CostEstimate(flops=flops, bytes_accessed=4 * 2**20, transcendentals=0),
        )(*args)

    return call


def bias_line(table):
    far = table[:, 2 * REL_CLIP :]
    near = table[:, 1:][:, ::-1]
    heads = table.shape[0]
    return jnp.concatenate(
        [
            jnp.broadcast_to(far, (heads, REACH - REL_CLIP)),
            near,
            table[:, :1],
            jnp.broadcast_to(far, (heads, Q_BLOCK - 1)),
        ],
        axis=1,
    )


def body(tokens, documents, norm_gain, w_query, w_key, w_value, w_out, rel_bias):
    rows, width = tokens.shape
    local = w_query.shape[2]
    core = lax.axis_index("c")
    x = lax.axis_index("x")
    z = lax.axis_index(("zh", "zl"))
    tp = lax.axis_index("tp")
    n_tp = lax.axis_size("tp")
    plane = ("x", "c")
    group = lax.axis_size(plane)
    bf = jnp.bfloat16

    piece = w_query.shape[1]
    ids = jnp.stack([core, x, z, tp])
    packed, rest = in_vmem(
        pack_kernel,
        [
            jax.ShapeDtypeStruct((group, piece, 3 * HEAD_DIM), bf),
            jax.ShapeDtypeStruct((group, piece, HEAD_DIM), bf),
        ],
        flops=10**8,
    )(ids, w_query[0], w_key[0], w_value[0], w_out[0].T)

    share = rows // n_tp
    at = lax.dynamic_slice_in_dim(tokens, tp * share, share, 0)
    line = bias_line(lax.dynamic_slice_in_dim(rel_bias[0], x * 2 + core, 1, 0))
    block = in_vmem(norm_kernel, jax.ShapeDtypeStruct((rows + 16, width), bf), flops=10**9)(
        tokens, norm_gain, documents[None, :]
    )
    swap = [(0, 1), (1, 0)]
    parts = [block, lax.ppermute(block, "c", swap)]
    mine = lax.all_to_all(packed, plane, 0, 0, tiled=True)
    mine = jnp.concatenate([mine, rest], axis=2).reshape(group * piece, 4 * HEAD_DIM)
    mine, line, at = lax.optimization_barrier((mine, line, at))
    for back in (1, 2, 3):
        got = lax.ppermute(block, "x", [(i, (i + back) % 4) for i in range(4)])
        parts += [got, lax.ppermute(got, "c", swap)]
    over_far = to_all(mine, "zh")
    w_in = to_all(over_far, "zl")
    rows_out = in_vmem(out_rows_kernel, jax.ShapeDtypeStruct((16 * piece, local), bf), flops=10**9)(w_in)
    w_mine = to_all(rows_out, "x")
    w_other = lax.ppermute(w_mine, "c", swap)
    qkv, docs, tail = in_vmem(
        qkv_kernel,
        [
            jax.ShapeDtypeStruct((group * rows, 4 * HEAD_DIM), bf),
            jax.ShapeDtypeStruct((group, rows), jnp.float32),
            jax.ShapeDtypeStruct((rows + 16, 4 * HEAD_DIM), bf),
        ],
        [pltpu.VMEM((width, 4 * HEAD_DIM), bf)],
        grant=24,
    )(ids, *parts, w_in)
    halo = lax.ppermute(tail, ("zh", "zl"), [(i, i + 1) for i in range(15)])
    att = in_vmem(attend_kernel, jax.ShapeDtypeStruct((group, rows // 2, 2 * HEAD_DIM), bf))(
        ids, qkv, halo, docs, line
    )
    att = lax.all_to_all(att, plane, 0, 0, tiled=True)
    partial = in_vmem(
        project_kernel,
        jax.ShapeDtypeStruct((rows, width), bf),
        [pltpu.VMEM((rows, local), bf), pltpu.VMEM((width, local), bf)],
    )(ids, att, w_mine, w_other)
    partial = lax.all_to_all(partial.reshape(n_tp, share, width), "tp", 0, 0, tiled=True)
    mixed = in_vmem(sum_kernel, jax.ShapeDtypeStruct((n_tp, share, width), bf), flops=10**8)(partial, at)
    return lax.all_to_all(mixed, "tp", 0, 0, tiled=True).reshape(rows, width)


def solution(mesh):
    split = Mesh(mesh.devices.reshape(4, 4, 4, 2, mesh.shape["tp"]), (*SP, "tp"))
    placed = (
        P(SP, None),
        P(SP),
        P(),
        P(None, SP, "tp"),
        P(None, SP, "tp"),
        P(None, SP, "tp"),
        P(None, None, SP),
        P(None, "tp", None),
    )

    def step(*args):
        return body(*args)

    step = jax.shard_map(step, mesh=split, in_specs=placed, out_specs=P(SP, None), check_vma=False)
    return step
```

```python
import jax
import jax.numpy as jnp
from jax import lax
from jax.experimental import pallas as pl
from jax.experimental.pallas import tpu as pltpu
from jax.sharding import Mesh
from jax.sharding import PartitionSpec as P

HEAD_DIM = 64
SEG = 64
LEFT = 4
REL_CLIP = 128
EPS = 1e-06
REACH = LEFT * SEG
Q_BLOCK = 2 * SEG
K_BLOCK = Q_BLOCK + REACH
SP = ("z", "x", "c")
NEG = -1e30


def to_all(x, axis):
    length = lax.axis_size(axis)
    return lax.all_to_all(jnp.broadcast_to(x[None], (length, *x.shape)), axis, 0, 0, tiled=True)


def pack_kernel(ids, w_q, w_k, w_v, w_o, heads, rest):
    n = heads.shape[0]
    own = w_o[:, pl.ds(pl.multiple_of(ids[3] * n * HEAD_DIM, n * HEAD_DIM), n * HEAD_DIM)]
    for i in range(n):
        cols = slice(i * HEAD_DIM, (i + 1) * HEAD_DIM)
        heads[i] = jnp.concatenate([w_q[:, cols], w_k[:, cols], w_v[:, cols]], axis=1)
        rest[i] = own[:, cols]


def sum_kernel(partial, tokens, out):
    total = tokens[...].astype(jnp.float32)
    for i in range(partial.shape[0]):
        total = total + partial[i].astype(jnp.float32)
    total = total.astype(jnp.bfloat16)
    for i in range(out.shape[0]):
        out[i] = total


def norm_kernel(tokens, gain, docs, out):
    rows = tokens.shape[0]
    wide = tokens[...].astype(jnp.float32)
    scale = lax.rsqrt(jnp.mean(wide * wide, axis=1, keepdims=True) + EPS)
    out[:rows, :] = (wide * scale * gain[...]).astype(jnp.bfloat16)
    extra = out.shape[0] - rows
    out[rows:, :rows] = jnp.broadcast_to(docs[...].astype(jnp.float32), (extra, rows)).astype(jnp.bfloat16)
    out[rows:, rows:] = jnp.zeros((extra, out.shape[1] - rows), jnp.bfloat16)


def qkv_kernel(ids, b0, s0, b1, s1, b2, s2, b3, s3, w_in, qkv, docs, tail):
    rows = qkv.shape[0] // 8
    weights = w_in[...].reshape(-1, w_in.shape[2])
    core, x = ids[0], ids[1]
    for back, pair in enumerate(((b0, s0), (b1, s1), (b2, s2), (b3, s3))):
        for c, part in zip((core, 1 - core), pair):
            at = ((x + 4 - back) & 3) * 2 + c
            total = jnp.dot(part[:rows, :], weights, preferred_element_type=jnp.float32)
            qkv[pl.ds(pl.multiple_of(at * rows, rows), rows), :] = total.astype(jnp.bfloat16)
            docs[pl.ds(at, 1), :] = part[rows : rows + 16, :rows].astype(jnp.float32)[0:1]
    tail[:rows, :] = qkv[7 * rows :, :]
    tail[rows:, :] = jnp.broadcast_to(docs[7:8, :], (16, rows)).astype(jnp.bfloat16)


def attend(blocks, ids, qkv, halo, docs, line, out):
    rows = docs.shape[1]
    flat = jnp.broadcast_to(line[...], (Q_BLOCK, line.shape[1]))
    bias = pltpu.roll(flat, 0, 1, stride=1, stride_axis=0)[:, :K_BLOCK]
    q_seg = lax.broadcasted_iota(jnp.int32, (Q_BLOCK, K_BLOCK), 0) // SEG
    k_seg = lax.broadcasted_iota(jnp.int32, (Q_BLOCK, K_BLOCK), 1) // SEG
    bias = jnp.where((k_seg >= q_seg) & (k_seg <= q_seg + LEFT), bias, NEG)
    if halo is not None:
        prior = jnp.where(ids[2] > 0, halo[rows : rows + 16, :].astype(jnp.float32)[0:1], -1.0)

    def doc_part(b):
        if b < 0:
            return prior[:, rows + b * Q_BLOCK : rows + (b + 1) * Q_BLOCK]
        at = b * Q_BLOCK % rows
        return docs[b * Q_BLOCK // rows : b * Q_BLOCK // rows + 1, at : at + Q_BLOCK]

    def row_part(b, cols):
        if b < 0:
            return halo[rows + b * Q_BLOCK : rows + (b + 1) * Q_BLOCK, cols]
        return qkv[b * Q_BLOCK : (b + 1) * Q_BLOCK, cols]

    def key_rows(b, cols):
        if b >= 2:
            return qkv[(b - 2) * Q_BLOCK : (b + 1) * Q_BLOCK, cols]
        return jnp.concatenate([row_part(i, cols) for i in range(b - 2, b + 1)], axis=0)

    for b in blocks:
        across = jnp.broadcast_to(doc_part(b), (Q_BLOCK, Q_BLOCK)).T
        same = jnp.concatenate([across == doc_part(i) for i in range(b - 2, b + 1)], axis=1)
        scores = lax.dot_general(
            qkv[b * Q_BLOCK : (b + 1) * Q_BLOCK, :HEAD_DIM],
            key_rows(b, slice(HEAD_DIM, 2 * HEAD_DIM)),
            (((1,), (1,)), ((), ())),
            preferred_element_type=jnp.float32,
        )
        scores = jnp.where(same, scores * HEAD_DIM ** (-0.5) + bias, NEG)
        peak = jnp.max(scores, axis=1, keepdims=True)
        raised = jnp.exp(scores - peak)
        total = jnp.sum(raised, axis=1, keepdims=True)
        mixed = jnp.dot(
            raised.astype(jnp.bfloat16),
            key_rows(b, slice(2 * HEAD_DIM, 3 * HEAD_DIM)),
            preferred_element_type=jnp.float32,
        )
        lane = b % 2 * HEAD_DIM
        out[b // 2, :, lane : lane + HEAD_DIM] = (mixed / total).astype(jnp.bfloat16)


def later_kernel(qkv, docs, line, out):
    out[0] = jnp.zeros(out.shape[1:], out.dtype)
    attend(range(2, qkv.shape[0] // Q_BLOCK), None, qkv, None, docs, line, out)


def early_kernel(ids, qkv, halo, docs, line, later, out):
    out[1:] = later[1:]
    attend(range(2), ids, qkv, halo, docs, line, out)


def out_rows_kernel(w_in, out):
    for z in range(w_in.shape[0]):
        out[16 * z : 16 * z + 16, :] = jnp.concatenate(
            [w_in[z, 16 * j : 16 * j + 16, 3 * HEAD_DIM :] for j in range(8)], axis=1
        )


def project_kernel(ids, att, w_mine, w_other, out, lhs, rhs):
    half = att.shape[1]
    for i in range(att.shape[0]):
        lhs[:half, i * HEAD_DIM : (i + 1) * HEAD_DIM] = att[i, :, :HEAD_DIM]
        lhs[half:, i * HEAD_DIM : (i + 1) * HEAD_DIM] = att[i, :, HEAD_DIM:]
    core = ids[0]
    for c, w in ((core, w_mine), (1 - core, w_other)):
        for z in range(16):
            for x in range(4):
                to = pl.multiple_of(z * 128 + x * 32 + c * 16, 16)
                rhs[pl.ds(to, 16), :] = w[x, z * 16 : z * 16 + 16, :]
    out[...] = lax.dot_general(
        lhs[...], rhs[...], (((1,), (1,)), ((), ())), preferred_element_type=jnp.float32
    ).astype(jnp.bfloat16)


def in_vmem(kernel, outs, scratch=(), grant=16, flops=2 * 10**10):
    one = not isinstance(outs, (list, tuple))
    shapes = [outs] if one else list(outs)
    specs = [pl.BlockSpec(memory_space=pltpu.VMEM) for _ in shapes]

    def call(*args):
        return pl.pallas_call(
            kernel,
            out_shape=shapes[0] if one else shapes,
            in_specs=[pl.BlockSpec(memory_space=pltpu.SMEM if a.ndim == 1 else pltpu.VMEM) for a in args],
            out_specs=specs[0] if one else specs,
            scratch_shapes=list(scratch),
            compiler_params=pltpu.CompilerParams(vmem_limit_bytes=grant * 2**20),
            cost_estimate=pl.CostEstimate(flops=flops, bytes_accessed=4 * 2**20, transcendentals=0),
        )(*args)

    return call


def bias_line(table):
    far = table[:, 2 * REL_CLIP :]
    near = table[:, 1:][:, ::-1]
    heads = table.shape[0]
    return jnp.concatenate(
        [
            jnp.broadcast_to(far, (heads, REACH - REL_CLIP)),
            near,
            table[:, :1],
            jnp.broadcast_to(far, (heads, Q_BLOCK - 1)),
        ],
        axis=1,
    )


def body(tokens, documents, norm_gain, w_query, w_key, w_value, w_out, rel_bias):
    rows, width = tokens.shape
    local = w_query.shape[2]
    core = lax.axis_index("c")
    x = lax.axis_index("x")
    z = lax.axis_index("z")
    tp = lax.axis_index("tp")
    n_tp = lax.axis_size("tp")
    plane = ("x", "c")
    group = lax.axis_size(plane)
    bf = jnp.bfloat16

    piece = w_query.shape[1]
    ids = jnp.stack([core, x, z, tp])
    packed, rest = in_vmem(
        pack_kernel,
        [
            jax.ShapeDtypeStruct((group, piece, 3 * HEAD_DIM), bf),
            jax.ShapeDtypeStruct((group, piece, HEAD_DIM), bf),
        ],
        flops=10**8,
    )(ids, w_query[0], w_key[0], w_value[0], w_out[0].T)

    share = rows // n_tp
    at = lax.dynamic_slice_in_dim(tokens, tp * share, share, 0)
    line = bias_line(lax.dynamic_slice_in_dim(rel_bias[0], x * 2 + core, 1, 0))
    block = in_vmem(norm_kernel, jax.ShapeDtypeStruct((rows + 16, width), bf), flops=10**9)(
        tokens, norm_gain, documents[None, :]
    )
    swap = [(0, 1), (1, 0)]
    parts = [block, lax.ppermute(block, "c", swap)]
    mine = lax.all_to_all(packed, plane, 0, 0, tiled=True)
    mine = jnp.concatenate([mine, rest], axis=2).reshape(group * piece, 4 * HEAD_DIM)
    for back in (1, 2, 3):
        got = lax.ppermute(block, "x", [(i, (i + back) % 4) for i in range(4)])
        parts += [got, lax.ppermute(got, "c", swap)]
    w_in = to_all(mine, "z")
    w_in, line, at = lax.optimization_barrier((w_in, line, at))
    rows_out = in_vmem(out_rows_kernel, jax.ShapeDtypeStruct((16 * piece, local), bf), flops=10**9)(w_in)
    w_mine = to_all(rows_out, "x")
    w_other = lax.ppermute(w_mine, "c", swap)
    qkv, docs, tail = in_vmem(
        qkv_kernel,
        [
            jax.ShapeDtypeStruct((group * rows, 4 * HEAD_DIM), bf),
            jax.ShapeDtypeStruct((group, rows), jnp.float32),
            jax.ShapeDtypeStruct((rows + 16, 4 * HEAD_DIM), bf),
        ],
        grant=24,
    )(ids, *parts, w_in)
    halo = lax.ppermute(tail, "z", [(i, i + 1) for i in range(15)])
    att_shape = jax.ShapeDtypeStruct((group, rows // 2, 2 * HEAD_DIM), bf)
    att = in_vmem(later_kernel, att_shape)(qkv, docs, line)
    att = in_vmem(early_kernel, att_shape, flops=10**9)(ids, qkv, halo, docs, line, att)
    att = lax.all_to_all(att, plane, 0, 0, tiled=True)
    partial = in_vmem(
        project_kernel,
        jax.ShapeDtypeStruct((rows, width), bf),
        [pltpu.VMEM((rows, local), bf), pltpu.VMEM((width, local), bf)],
    )(ids, att, w_mine, w_other)
    partial = lax.all_to_all(partial.reshape(n_tp, share, width), "tp", 0, 0, tiled=True)
    mixed = in_vmem(sum_kernel, jax.ShapeDtypeStruct((n_tp, share, width), bf), flops=10**8)(partial, at)
    return lax.all_to_all(mixed, "tp", 0, 0, tiled=True).reshape(rows, width)


def solution(mesh):
    split = Mesh(mesh.devices.reshape(16, 4, 2, mesh.shape["tp"]), (*SP, "tp"))
    placed = (
        P(SP, None),
        P(SP),
        P(),
        P(None, SP, "tp"),
        P(None, SP, "tp"),
        P(None, SP, "tp"),
        P(None, None, SP),
        P(None, "tp", None),
    )

    def step(*args):
        return body(*args)

    step = jax.shard_map(step, mesh=split, in_specs=placed, out_specs=P(SP, None), check_vma=False)
    return step
```

```python
import jax
import jax.numpy as jnp
from jax import lax
from jax.experimental import pallas as pl
from jax.experimental.pallas import tpu as pltpu
from jax.sharding import Mesh
from jax.sharding import PartitionSpec as P

HEAD_DIM = 64
SEG = 64
LEFT = 4
REL_CLIP = 128
EPS = 1e-06
REACH = LEFT * SEG
Q_BLOCK = 2 * SEG
K_BLOCK = Q_BLOCK + REACH
SP = ("zh", "zl", "x", "c")
Z = ("zh", "zl")
NEG = -1e30


def to_all(x, axis):
    length = lax.axis_size(axis)
    return lax.all_to_all(jnp.broadcast_to(x[None], (length, *x.shape)), axis, 0, 0, tiled=True)


def prep_kernel(ids, w_q, w_k, w_v, w_o, tokens, gain, docs, heads, rest, block):
    n = heads.shape[0]
    own = w_o[:, pl.ds(pl.multiple_of(ids[3] * n * HEAD_DIM, n * HEAD_DIM), n * HEAD_DIM)]
    for i in range(n):
        cols = slice(i * HEAD_DIM, (i + 1) * HEAD_DIM)
        heads[i] = jnp.concatenate([w_q[:, cols], w_k[:, cols], w_v[:, cols]], axis=1)
        rest[i] = own[:, cols]
    rows = tokens.shape[0]
    wide = tokens[...].astype(jnp.float32)
    scale = lax.rsqrt(jnp.mean(wide * wide, axis=1, keepdims=True) + EPS)
    block[:rows, :] = (wide * scale * gain[...]).astype(jnp.bfloat16)
    extra = block.shape[0] - rows
    block[rows:, :rows] = jnp.broadcast_to(docs[...].astype(jnp.float32), (extra, rows)).astype(jnp.bfloat16)
    block[rows:, rows:] = jnp.zeros((extra, block.shape[1] - rows), jnp.bfloat16)


def sum_kernel(partial, tokens, out):
    total = tokens[...].astype(jnp.float32)
    for i in range(partial.shape[0]):
        total = total + partial[i].astype(jnp.float32)
    total = total.astype(jnp.bfloat16)
    for i in range(out.shape[0]):
        out[i] = total


def qkv_kernel(ids, b0, s0, b1, s1, b2, s2, b3, s3, w_in, qkv, docs, tail):
    rows = qkv.shape[0] // 8
    core, x = ids[0], ids[1]
    for back, pair in enumerate(((b0, s0), (b1, s1), (b2, s2), (b3, s3))):
        for c, part in zip((core, 1 - core), pair):
            at = ((x + 4 - back) & 3) * 2 + c
            total = jnp.dot(part[:rows, :], w_in[...], preferred_element_type=jnp.float32)
            qkv[pl.ds(pl.multiple_of(at * rows, rows), rows), :] = total.astype(jnp.bfloat16)
            docs[pl.ds(at, 1), :] = part[rows : rows + 16, :rows].astype(jnp.float32)[0:1]
    tail[:rows, :] = qkv[7 * rows :, :]
    tail[rows:, :] = jnp.broadcast_to(docs[7:8, :], (16, rows)).astype(jnp.bfloat16)


def attend(blocks, ids, qkv, halo, docs, line, out):
    rows = docs.shape[1]
    flat = jnp.broadcast_to(line[...], (Q_BLOCK, line.shape[1]))
    bias = pltpu.roll(flat, 0, 1, stride=1, stride_axis=0)[:, :K_BLOCK]
    q_seg = lax.broadcasted_iota(jnp.int32, (Q_BLOCK, K_BLOCK), 0) // SEG
    k_seg = lax.broadcasted_iota(jnp.int32, (Q_BLOCK, K_BLOCK), 1) // SEG
    bias = jnp.where((k_seg >= q_seg) & (k_seg <= q_seg + LEFT), bias, NEG)
    if halo is not None:
        prior = jnp.where(ids[2] > 0, halo[rows : rows + 16, :].astype(jnp.float32)[0:1], -1.0)

    def doc_part(b):
        if b < 0:
            return prior[:, rows + b * Q_BLOCK : rows + (b + 1) * Q_BLOCK]
        at = b * Q_BLOCK % rows
        return docs[b * Q_BLOCK // rows : b * Q_BLOCK // rows + 1, at : at + Q_BLOCK]

    def row_part(b, cols):
        if b < 0:
            return halo[rows + b * Q_BLOCK : rows + (b + 1) * Q_BLOCK, cols]
        return qkv[b * Q_BLOCK : (b + 1) * Q_BLOCK, cols]

    def key_rows(b, cols):
        if b >= 2:
            return qkv[(b - 2) * Q_BLOCK : (b + 1) * Q_BLOCK, cols]
        return jnp.concatenate([row_part(i, cols) for i in range(b - 2, b + 1)], axis=0)

    for b in blocks:
        across = jnp.broadcast_to(doc_part(b), (Q_BLOCK, Q_BLOCK)).T
        same = jnp.concatenate([across == doc_part(i) for i in range(b - 2, b + 1)], axis=1)
        scores = lax.dot_general(
            qkv[b * Q_BLOCK : (b + 1) * Q_BLOCK, :HEAD_DIM],
            key_rows(b, slice(HEAD_DIM, 2 * HEAD_DIM)),
            (((1,), (1,)), ((), ())),
            preferred_element_type=jnp.float32,
        )
        scores = jnp.where(same, scores * HEAD_DIM ** (-0.5) + bias, NEG)
        peak = jnp.max(scores, axis=1, keepdims=True)
        raised = jnp.exp(scores - peak)
        total = jnp.sum(raised, axis=1, keepdims=True)
        mixed = jnp.dot(
            raised.astype(jnp.bfloat16),
            key_rows(b, slice(2 * HEAD_DIM, 3 * HEAD_DIM)),
            preferred_element_type=jnp.float32,
        )
        lane = b % 2 * HEAD_DIM
        out[b // 2, :, lane : lane + HEAD_DIM] = (mixed / total).astype(jnp.bfloat16)


def later_kernel(qkv, docs, line, out):
    out[0] = jnp.zeros(out.shape[1:], out.dtype)
    attend(range(2, qkv.shape[0] // Q_BLOCK), None, qkv, None, docs, line, out)


def early_kernel(ids, qkv, halo, docs, line, later, out):
    out[1:] = later[1:]
    attend(range(2), ids, qkv, halo, docs, line, out)


def order_kernel(ids, own, below, above, low, high, w_all, rows_out):
    lanes = own.shape[1]
    for ahead, part, first in ((0, own, 0), (3, below, 0), (1, above, 0), (2, low, 0), (2, high, low.shape[0])):
        for i in range(part.shape[0]):
            z = (first + i) * 4 + ((ids[2] + ahead) & 3)
            w_all[pl.ds(pl.multiple_of(z * lanes, lanes), lanes), :] = part[i]
            rows_out[pl.ds(pl.multiple_of(z * 16, 16), 16), :] = jnp.concatenate(
                [part[i, 16 * j : 16 * j + 16, 3 * HEAD_DIM :] for j in range(8)], axis=1
            )


def project_kernel(ids, att, w_mine, w_other, out, lhs, rhs):
    half = att.shape[1]
    for i in range(att.shape[0]):
        lhs[:half, i * HEAD_DIM : (i + 1) * HEAD_DIM] = att[i, :, :HEAD_DIM]
        lhs[half:, i * HEAD_DIM : (i + 1) * HEAD_DIM] = att[i, :, HEAD_DIM:]
    core = ids[0]
    for c, w in ((core, w_mine), (1 - core, w_other)):
        for z in range(16):
            for x in range(4):
                to = pl.multiple_of(z * 128 + x * 32 + c * 16, 16)
                rhs[pl.ds(to, 16), :] = w[x, z * 16 : z * 16 + 16, :]
    out[...] = lax.dot_general(
        lhs[...], rhs[...], (((1,), (1,)), ((), ())), preferred_element_type=jnp.float32
    ).astype(jnp.bfloat16)


def in_vmem(kernel, outs, scratch=(), grant=16, flops=2 * 10**10):
    one = not isinstance(outs, (list, tuple))
    shapes = [outs] if one else list(outs)
    specs = [pl.BlockSpec(memory_space=pltpu.VMEM) for _ in shapes]

    def call(*args):
        return pl.pallas_call(
            kernel,
            out_shape=shapes[0] if one else shapes,
            in_specs=[pl.BlockSpec(memory_space=pltpu.SMEM if a.ndim == 1 else pltpu.VMEM) for a in args],
            out_specs=specs[0] if one else specs,
            scratch_shapes=list(scratch),
            compiler_params=pltpu.CompilerParams(vmem_limit_bytes=grant and grant * 2**20),
            cost_estimate=pl.CostEstimate(flops=flops, bytes_accessed=4 * 2**20, transcendentals=0),
        )(*args)

    return call


def bias_line(table):
    far = table[:, 2 * REL_CLIP :]
    near = table[:, 1:][:, ::-1]
    heads = table.shape[0]
    return jnp.concatenate(
        [
            jnp.broadcast_to(far, (heads, REACH - REL_CLIP)),
            near,
            table[:, :1],
            jnp.broadcast_to(far, (heads, Q_BLOCK - 1)),
        ],
        axis=1,
    )


def body(tokens, documents, norm_gain, w_query, w_key, w_value, w_out, rel_bias):
    rows, width = tokens.shape
    local = w_query.shape[2]
    core = lax.axis_index("c")
    x = lax.axis_index("x")
    z = lax.axis_index(Z)
    tp = lax.axis_index("tp")
    n_tp = lax.axis_size("tp")
    plane = ("x", "c")
    group = lax.axis_size(plane)
    bf = jnp.bfloat16

    piece = w_query.shape[1]
    ids = jnp.stack([core, x, z, tp])
    sources = (w_query[0], w_key[0], w_value[0], w_out[0].T, tokens, norm_gain, documents[None, :])
    packed, rest, block = in_vmem(
        prep_kernel,
        [
            jax.ShapeDtypeStruct((group, piece, 3 * HEAD_DIM), bf),
            jax.ShapeDtypeStruct((group, piece, HEAD_DIM), bf),
            jax.ShapeDtypeStruct((rows + 16, width), bf),
        ],
        grant=None,
        flops=10**9,
    )(ids, *sources)

    share = rows // n_tp
    at = lax.dynamic_slice_in_dim(tokens, tp * share, share, 0)
    line = bias_line(lax.dynamic_slice_in_dim(rel_bias[0], x * 2 + core, 1, 0))
    swap = [(0, 1), (1, 0)]
    parts = [block, lax.ppermute(block, "c", swap)]
    mine = lax.all_to_all(packed, plane, 0, 0, tiled=True)
    mine = jnp.concatenate([mine, rest], axis=2).reshape(group * piece, 4 * HEAD_DIM)
    for back in (1, 2, 3):
        got = lax.ppermute(block, "x", [(i, (i + back) % 4) for i in range(4)])
        parts += [got, lax.ppermute(got, "c", swap)]
    over_far = to_all(mine, "zh")
    over_far, line, at = lax.optimization_barrier((over_far, line, at))
    near = []
    two = over_far.shape[0] // 2
    for by, part in ((1, over_far), (-1, over_far), (2, over_far[:two]), (-2, over_far[two:])):
        near.append(lax.ppermute(part, Z, [(n, (n + by) % 16) for n in range(16)]))
    w_in, rows_out = in_vmem(
        order_kernel,
        [
            jax.ShapeDtypeStruct((width, 4 * HEAD_DIM), bf),
            jax.ShapeDtypeStruct((16 * piece, local), bf),
        ],
        flops=10**9,
    )(ids, over_far, *near)
    w_mine = to_all(rows_out, "x")
    w_other = lax.ppermute(w_mine, "c", swap)
    qkv, docs, tail = in_vmem(
        qkv_kernel,
        [
            jax.ShapeDtypeStruct((group * rows, 4 * HEAD_DIM), bf),
            jax.ShapeDtypeStruct((group, rows), jnp.float32),
            jax.ShapeDtypeStruct((rows + 16, 4 * HEAD_DIM), bf),
        ],
        grant=None,
    )(ids, *parts, w_in)
    halo = lax.ppermute(tail, Z, [(i, i + 1) for i in range(15)])
    att_shape = jax.ShapeDtypeStruct((group, rows // 2, 2 * HEAD_DIM), bf)
    att = in_vmem(later_kernel, att_shape)(qkv, docs, line)
    att = in_vmem(early_kernel, att_shape, flops=10**9)(ids, qkv, halo, docs, line, att)
    att = lax.all_to_all(att, plane, 0, 0, tiled=True)
    partial = in_vmem(
        project_kernel,
        jax.ShapeDtypeStruct((rows, width), bf),
        [pltpu.VMEM((rows, local), bf), pltpu.VMEM((width, local), bf)],
    )(ids, att, w_mine, w_other)
    partial = lax.all_to_all(partial.reshape(n_tp, share, width), "tp", 0, 0, tiled=True)
    mixed = in_vmem(sum_kernel, jax.ShapeDtypeStruct((n_tp, share, width), bf), flops=10**8)(partial, at)
    return lax.all_to_all(mixed, "tp", 0, 0, tiled=True).reshape(rows, width)


def solution(mesh):
    split = Mesh(mesh.devices.reshape(4, 4, 4, 2, mesh.shape["tp"]), (*SP, "tp"))
    placed = (
        P(SP, None),
        P(SP),
        P(),
        P(None, SP, "tp"),
        P(None, SP, "tp"),
        P(None, SP, "tp"),
        P(None, None, SP),
        P(None, "tp", None),
    )

    def step(*args):
        return body(*args)

    step = jax.shard_map(step, mesh=split, in_specs=placed, out_specs=P(SP, None), check_vma=False)
    return step
```

```python
import jax
import jax.numpy as jnp
from jax import lax
from jax.experimental import pallas as pl
from jax.experimental.pallas import tpu as pltpu
from jax.sharding import Mesh
from jax.sharding import PartitionSpec as P

HEAD_DIM = 64
SEG = 64
LEFT = 4
REL_CLIP = 128
EPS = 1e-06
REACH = LEFT * SEG
Q_BLOCK = 2 * SEG
K_BLOCK = Q_BLOCK + REACH
SP = ("zh", "zl", "x", "c")
Z = ("zh", "zl")
NEG = -1e30


def to_all(x, axis):
    length = lax.axis_size(axis)
    return lax.all_to_all(jnp.broadcast_to(x[None], (length, *x.shape)), axis, 0, 0, tiled=True)


def prep_kernel(ids, w_q, w_k, w_v, w_o, tokens, gain, docs, heads, rest, block):
    n = heads.shape[0]
    own = w_o[:, pl.ds(pl.multiple_of(ids[3] * n * HEAD_DIM, n * HEAD_DIM), n * HEAD_DIM)]
    for i in range(n):
        cols = slice(i * HEAD_DIM, (i + 1) * HEAD_DIM)
        heads[i] = jnp.concatenate([w_q[:, cols], w_k[:, cols], w_v[:, cols]], axis=1)
        rest[i] = own[:, cols]
    rows = tokens.shape[0]
    wide = tokens[...].astype(jnp.float32)
    scale = lax.rsqrt(jnp.mean(wide * wide, axis=1, keepdims=True) + EPS)
    block[:rows, :] = (wide * scale * gain[...]).astype(jnp.bfloat16)
    extra = block.shape[0] - rows
    block[rows:, :rows] = jnp.broadcast_to(docs[...].astype(jnp.float32), (extra, rows)).astype(jnp.bfloat16)
    block[rows:, rows:] = jnp.zeros((extra, block.shape[1] - rows), jnp.bfloat16)


def sum_kernel(partial, tokens, out):
    total = tokens[...].astype(jnp.float32)
    for i in range(partial.shape[0]):
        total = total + partial[i].astype(jnp.float32)
    total = total.astype(jnp.bfloat16)
    for i in range(out.shape[0]):
        out[i] = total


def qkv_kernel(ids, b0, s0, b1, s1, b2, s2, b3, s3, w_in, qkv, docs, tail, head):
    rows = qkv.shape[0] // 8
    core, x = ids[0], ids[1]
    for back, pair in enumerate(((b0, s0), (b1, s1), (b2, s2), (b3, s3))):
        for c, part in zip((core, 1 - core), pair):
            at = ((x + 4 - back) & 3) * 2 + c
            total = jnp.dot(part[:rows, :], w_in[...], preferred_element_type=jnp.float32)
            qkv[pl.ds(pl.multiple_of(at * rows, rows), rows), :] = total.astype(jnp.bfloat16)
            docs[pl.ds(at, 1), :] = part[rows : rows + 16, :rows].astype(jnp.float32)[0:1]
    head[...] = qkv[:rows, :]
    tail[:rows, :] = qkv[7 * rows :, :]
    tail[rows:, :] = jnp.broadcast_to(docs[7:8, :], (16, rows)).astype(jnp.bfloat16)


def attend(blocks, ids, qkv, halo, docs, line, out):
    rows = docs.shape[1]
    flat = jnp.broadcast_to(line[...], (Q_BLOCK, line.shape[1]))
    bias = pltpu.roll(flat, 0, 1, stride=1, stride_axis=0)[:, :K_BLOCK]
    q_seg = lax.broadcasted_iota(jnp.int32, (Q_BLOCK, K_BLOCK), 0) // SEG
    k_seg = lax.broadcasted_iota(jnp.int32, (Q_BLOCK, K_BLOCK), 1) // SEG
    bias = jnp.where((k_seg >= q_seg) & (k_seg <= q_seg + LEFT), bias, NEG)
    if halo is not None:
        prior = jnp.where(ids[2] > 0, halo[rows : rows + 16, :].astype(jnp.float32)[0:1], -1.0)

    def doc_part(b):
        if b < 0:
            return prior[:, rows + b * Q_BLOCK : rows + (b + 1) * Q_BLOCK]
        at = b * Q_BLOCK % rows
        return docs[b * Q_BLOCK // rows : b * Q_BLOCK // rows + 1, at : at + Q_BLOCK]

    def row_part(b, cols):
        if b < 0:
            return halo[rows + b * Q_BLOCK : rows + (b + 1) * Q_BLOCK, cols]
        return qkv[b * Q_BLOCK : (b + 1) * Q_BLOCK, cols]

    def key_rows(b, cols):
        if b >= 2:
            return qkv[(b - 2) * Q_BLOCK : (b + 1) * Q_BLOCK, cols]
        return jnp.concatenate([row_part(i, cols) for i in range(b - 2, b + 1)], axis=0)

    for b in blocks:
        across = jnp.broadcast_to(doc_part(b), (Q_BLOCK, Q_BLOCK)).T
        same = jnp.concatenate([across == doc_part(i) for i in range(b - 2, b + 1)], axis=1)
        scores = lax.dot_general(
            qkv[b * Q_BLOCK : (b + 1) * Q_BLOCK, :HEAD_DIM],
            key_rows(b, slice(HEAD_DIM, 2 * HEAD_DIM)),
            (((1,), (1,)), ((), ())),
            preferred_element_type=jnp.float32,
        )
        scores = jnp.where(same, scores * HEAD_DIM ** (-0.5) + bias, NEG)
        peak = jnp.max(scores, axis=1, keepdims=True)
        raised = jnp.exp(scores - peak)
        total = jnp.sum(raised, axis=1, keepdims=True)
        mixed = jnp.dot(
            raised.astype(jnp.bfloat16),
            key_rows(b, slice(2 * HEAD_DIM, 3 * HEAD_DIM)),
            preferred_element_type=jnp.float32,
        )
        lane = b % 2 * HEAD_DIM
        out[b // 2, :, lane : lane + HEAD_DIM] = (mixed / total).astype(jnp.bfloat16)


def later_kernel(qkv, docs, line, out):
    out[0] = jnp.zeros(out.shape[1:], out.dtype)
    attend(range(2, qkv.shape[0] // Q_BLOCK), None, qkv, None, docs, line, out)


def early_kernel(ids, qkv, halo, docs, line, later, out):
    out[1:] = later[1:]
    attend(range(2), ids, qkv, halo, docs, line, out)


def order_kernel(ids, own, below, above, second, w_all, rows_out):
    lanes = own.shape[1]
    for ahead, part in ((0, own), (3, below), (1, above), (2, second)):
        for i in range(part.shape[0]):
            z = i * 4 + ((ids[2] + ahead) & 3)
            w_all[pl.ds(pl.multiple_of(z * lanes, lanes), lanes), :] = part[i]
            rows_out[pl.ds(pl.multiple_of(z * 16, 16), 16), :] = jnp.concatenate(
                [part[i, 16 * j : 16 * j + 16, 3 * HEAD_DIM :] for j in range(8)], axis=1
            )


def project_kernel(ids, att, w_mine, w_other, out, lhs, rhs):
    half = att.shape[1]
    for i in range(att.shape[0]):
        lhs[:half, i * HEAD_DIM : (i + 1) * HEAD_DIM] = att[i, :, :HEAD_DIM]
        lhs[half:, i * HEAD_DIM : (i + 1) * HEAD_DIM] = att[i, :, HEAD_DIM:]
    core = ids[0]
    for c, w in ((core, w_mine), (1 - core, w_other)):
        for z in range(16):
            for x in range(4):
                to = pl.multiple_of(z * 128 + x * 32 + c * 16, 16)
                rhs[pl.ds(to, 16), :] = w[x, z * 16 : z * 16 + 16, :]
    out[...] = lax.dot_general(
        lhs[...], rhs[...], (((1,), (1,)), ((), ())), preferred_element_type=jnp.float32
    ).astype(jnp.bfloat16)


def in_vmem(kernel, outs, scratch=(), grant=16, flops=2 * 10**10):
    one = not isinstance(outs, (list, tuple))
    shapes = [outs] if one else list(outs)
    specs = [pl.BlockSpec(memory_space=pltpu.VMEM) for _ in shapes]

    def call(*args):
        return pl.pallas_call(
            kernel,
            out_shape=shapes[0] if one else shapes,
            in_specs=[pl.BlockSpec(memory_space=pltpu.SMEM if a.ndim == 1 else pltpu.VMEM) for a in args],
            out_specs=specs[0] if one else specs,
            scratch_shapes=list(scratch),
            compiler_params=pltpu.CompilerParams(vmem_limit_bytes=grant and grant * 2**20),
            cost_estimate=pl.CostEstimate(flops=flops, bytes_accessed=4 * 2**20, transcendentals=0),
        )(*args)

    return call


def bias_line(table):
    far = table[:, 2 * REL_CLIP :]
    near = table[:, 1:][:, ::-1]
    heads = table.shape[0]
    return jnp.concatenate(
        [
            jnp.broadcast_to(far, (heads, REACH - REL_CLIP)),
            near,
            table[:, :1],
            jnp.broadcast_to(far, (heads, Q_BLOCK - 1)),
        ],
        axis=1,
    )


def body(tokens, documents, norm_gain, w_query, w_key, w_value, w_out, rel_bias):
    rows, width = tokens.shape
    local = w_query.shape[2]
    core = lax.axis_index("c")
    x = lax.axis_index("x")
    z = lax.axis_index(Z)
    tp = lax.axis_index("tp")
    n_tp = lax.axis_size("tp")
    plane = ("x", "c")
    group = lax.axis_size(plane)
    bf = jnp.bfloat16

    piece = w_query.shape[1]
    ids = jnp.stack([core, x, z, tp])
    sources = (w_query[0], w_key[0], w_value[0], w_out[0].T, tokens, norm_gain, documents[None, :])
    packed, rest, block = in_vmem(
        prep_kernel,
        [
            jax.ShapeDtypeStruct((group, piece, 3 * HEAD_DIM), bf),
            jax.ShapeDtypeStruct((group, piece, HEAD_DIM), bf),
            jax.ShapeDtypeStruct((rows + 16, width), bf),
        ],
        grant=None,
        flops=10**9,
    )(ids, *sources)

    share = rows // n_tp
    at = lax.dynamic_slice_in_dim(tokens, tp * share, share, 0)
    line = bias_line(lax.dynamic_slice_in_dim(rel_bias[0], x * 2 + core, 1, 0))
    swap = [(0, 1), (1, 0)]
    parts = [block, lax.ppermute(block, "c", swap)]
    mine = lax.all_to_all(packed, plane, 0, 0, tiled=True)
    mine = jnp.concatenate([mine, rest], axis=2).reshape(group * piece, 4 * HEAD_DIM)
    for back in (1, 2, 3):
        got = lax.ppermute(block, "x", [(i, (i + back) % 4) for i in range(4)])
        parts += [got, lax.ppermute(got, "c", swap)]
    over_far = to_all(mine, "zh")
    over_far, line, at = lax.optimization_barrier((over_far, line, at))
    near = []
    for by in (1, -1, 2):
        near.append(lax.ppermute(over_far, Z, [(n, (n + by) % 16) for n in range(16)]))
    w_in, rows_out = in_vmem(
        order_kernel,
        [
            jax.ShapeDtypeStruct((width, 4 * HEAD_DIM), bf),
            jax.ShapeDtypeStruct((16 * piece, local), bf),
        ],
        flops=10**9,
    )(ids, over_far, *near)
    w_mine = to_all(rows_out, "x")
    w_other = lax.ppermute(w_mine, "c", swap)
    qkv, docs, tail, head = in_vmem(
        qkv_kernel,
        [
            jax.ShapeDtypeStruct((group * rows, 4 * HEAD_DIM), bf),
            jax.ShapeDtypeStruct((group, rows), jnp.float32),
            jax.ShapeDtypeStruct((rows + 16, 4 * HEAD_DIM), bf),
            jax.ShapeDtypeStruct((rows, 4 * HEAD_DIM), bf),
        ],
        grant=24,
    )(ids, *parts, w_in)
    halo = lax.ppermute(tail, Z, [(i, i + 1) for i in range(15)])
    att_shape = jax.ShapeDtypeStruct((group, rows // 2, 2 * HEAD_DIM), bf)
    att = in_vmem(later_kernel, att_shape)(qkv, docs, line)
    att = in_vmem(early_kernel, att_shape, flops=10**9)(ids, head, halo, docs, line, att)
    att = lax.all_to_all(att, plane, 0, 0, tiled=True)
    partial = in_vmem(
        project_kernel,
        jax.ShapeDtypeStruct((rows, width), bf),
        [pltpu.VMEM((rows, local), bf), pltpu.VMEM((width, local), bf)],
    )(ids, att, w_mine, w_other)
    partial = lax.all_to_all(partial.reshape(n_tp, share, width), "tp", 0, 0, tiled=True)
    mixed = in_vmem(sum_kernel, jax.ShapeDtypeStruct((n_tp, share, width), bf), flops=10**8)(partial, at)
    return lax.all_to_all(mixed, "tp", 0, 0, tiled=True).reshape(rows, width)


def solution(mesh):
    split = Mesh(mesh.devices.reshape(4, 4, 4, 2, mesh.shape["tp"]), (*SP, "tp"))
    placed = (
        P(SP, None),
        P(SP),
        P(),
        P(None, SP, "tp"),
        P(None, SP, "tp"),
        P(None, SP, "tp"),
        P(None, None, SP),
        P(None, "tp", None),
    )

    def step(*args):
        return body(*args)

    step = jax.shard_map(step, mesh=split, in_specs=placed, out_specs=P(SP, None), check_vma=False)
    return step
```

```python
import jax
import jax.numpy as jnp
from jax import lax
from jax.experimental import pallas as pl
from jax.experimental.pallas import tpu as pltpu
from jax.sharding import Mesh
from jax.sharding import PartitionSpec as P

HEAD_DIM = 64
SEG = 64
LEFT = 4
REL_CLIP = 128
EPS = 1e-06
REACH = LEFT * SEG
Q_BLOCK = 2 * SEG
K_BLOCK = Q_BLOCK + REACH
SP = ("zh", "zl", "x", "c")
Z = ("zh", "zl")
NEG = -1e30


def to_all(x, axis):
    length = lax.axis_size(axis)
    return lax.all_to_all(jnp.broadcast_to(x[None], (length, *x.shape)), axis, 0, 0, tiled=True)


def prep_kernel(ids, w_q, w_k, w_v, w_o, tokens, gain, docs, heads, block):
    n = heads.shape[0]
    own = w_o[:, pl.ds(pl.multiple_of(ids[3] * n * HEAD_DIM, n * HEAD_DIM), n * HEAD_DIM)]
    for i in range(n):
        cols = slice(i * HEAD_DIM, (i + 1) * HEAD_DIM)
        heads[i] = jnp.concatenate([w_q[:, cols], w_k[:, cols], w_v[:, cols], own[:, cols]], axis=1)
    rows = tokens.shape[0]
    wide = tokens[...].astype(jnp.float32)
    scale = lax.rsqrt(jnp.mean(wide * wide, axis=1, keepdims=True) + EPS)
    block[:rows, :] = (wide * scale * gain[...]).astype(jnp.bfloat16)
    extra = block.shape[0] - rows
    block[rows:, :rows] = jnp.broadcast_to(docs[...].astype(jnp.float32), (extra, rows)).astype(jnp.bfloat16)
    block[rows:, rows:] = jnp.zeros((extra, block.shape[1] - rows), jnp.bfloat16)


def sum_kernel(partial, tokens, out):
    total = tokens[...].astype(jnp.float32)
    for i in range(partial.shape[0]):
        total = total + partial[i].astype(jnp.float32)
    total = total.astype(jnp.bfloat16)
    for i in range(out.shape[0]):
        out[i] = total


def qkv_kernel(ids, b0, s0, b1, s1, b2, s2, b3, s3, w_in, qkv, docs, tail, head):
    rows = qkv.shape[0] // 8
    core, x = ids[0], ids[1]
    for back, pair in enumerate(((b0, s0), (b1, s1), (b2, s2), (b3, s3))):
        for c, part in zip((core, 1 - core), pair):
            at = ((x + 4 - back) & 3) * 2 + c
            total = jnp.dot(part[:rows, :], w_in[...], preferred_element_type=jnp.float32)
            qkv[pl.ds(pl.multiple_of(at * rows, rows), rows), :] = total.astype(jnp.bfloat16)
            docs[pl.ds(at, 1), :] = part[rows : rows + 16, :rows].astype(jnp.float32)[0:1]
    head[...] = qkv[:rows, :]
    tail[:rows, :] = qkv[7 * rows :, :]
    tail[rows:, :] = jnp.broadcast_to(docs[7:8, :], (16, rows)).astype(jnp.bfloat16)


def attend(blocks, ids, qkv, halo, docs, line, out):
    rows = docs.shape[1]
    flat = jnp.broadcast_to(line[...], (Q_BLOCK, line.shape[1]))
    bias = pltpu.roll(flat, 0, 1, stride=1, stride_axis=0)[:, :K_BLOCK]
    q_seg = lax.broadcasted_iota(jnp.int32, (Q_BLOCK, K_BLOCK), 0) // SEG
    k_seg = lax.broadcasted_iota(jnp.int32, (Q_BLOCK, K_BLOCK), 1) // SEG
    bias = jnp.where((k_seg >= q_seg) & (k_seg <= q_seg + LEFT), bias, NEG)
    if halo is not None:
        prior = jnp.where(ids[2] > 0, halo[rows : rows + 16, :].astype(jnp.float32)[0:1], -1.0)

    def doc_part(b):
        if b < 0:
            return prior[:, rows + b * Q_BLOCK : rows + (b + 1) * Q_BLOCK]
        at = b * Q_BLOCK % rows
        return docs[b * Q_BLOCK // rows : b * Q_BLOCK // rows + 1, at : at + Q_BLOCK]

    def row_part(b, cols):
        if b < 0:
            return halo[rows + b * Q_BLOCK : rows + (b + 1) * Q_BLOCK, cols]
        return qkv[b * Q_BLOCK : (b + 1) * Q_BLOCK, cols]

    def key_rows(b, cols):
        if b >= 2:
            return qkv[(b - 2) * Q_BLOCK : (b + 1) * Q_BLOCK, cols]
        return jnp.concatenate([row_part(i, cols) for i in range(b - 2, b + 1)], axis=0)

    for b in blocks:
        across = jnp.broadcast_to(doc_part(b), (Q_BLOCK, Q_BLOCK)).T
        same = jnp.concatenate([across == doc_part(i) for i in range(b - 2, b + 1)], axis=1)
        scores = lax.dot_general(
            qkv[b * Q_BLOCK : (b + 1) * Q_BLOCK, :HEAD_DIM],
            key_rows(b, slice(HEAD_DIM, 2 * HEAD_DIM)),
            (((1,), (1,)), ((), ())),
            preferred_element_type=jnp.float32,
        )
        scores = jnp.where(same, scores * HEAD_DIM ** (-0.5) + bias, NEG)
        peak = jnp.max(scores, axis=1, keepdims=True)
        raised = jnp.exp(scores - peak)
        total = jnp.sum(raised, axis=1, keepdims=True)
        mixed = jnp.dot(
            raised.astype(jnp.bfloat16),
            key_rows(b, slice(2 * HEAD_DIM, 3 * HEAD_DIM)),
            preferred_element_type=jnp.float32,
        )
        lane = b % 2 * HEAD_DIM
        out[b // 2, :, lane : lane + HEAD_DIM] = (mixed / total).astype(jnp.bfloat16)


def later_kernel(qkv, docs, line, out):
    out[0] = jnp.zeros(out.shape[1:], out.dtype)
    attend(range(2, qkv.shape[0] // Q_BLOCK), None, qkv, None, docs, line, out)


def early_kernel(ids, qkv, halo, docs, line, later, out):
    out[1:] = later[1:]
    attend(range(2), ids, qkv, halo, docs, line, out)


def order_kernel(ids, own, below, above, second, w_all, rows_out):
    lanes = own.shape[1]
    for ahead, part in ((0, own), (3, below), (1, above), (2, second)):
        for i in range(part.shape[0]):
            z = i * 4 + ((ids[2] + ahead) & 3)
            w_all[pl.ds(pl.multiple_of(z * lanes, lanes), lanes), :] = part[i]
    half = rows_out.shape[0]
    rows_out[...] = jnp.concatenate([w_all[:half, 3 * HEAD_DIM :], w_all[half:, 3 * HEAD_DIM :]], axis=1)


def project_kernel(ids, att, w_mine, w_other, out, lhs, rhs):
    half = att.shape[1]
    for i in range(att.shape[0]):
        lhs[:half, i * HEAD_DIM : (i + 1) * HEAD_DIM] = att[i, :, :HEAD_DIM]
        lhs[half:, i * HEAD_DIM : (i + 1) * HEAD_DIM] = att[i, :, HEAD_DIM:]
    core = ids[0]
    cut = w_mine.shape[1]
    for x in range(w_mine.shape[0]):
        pair = [jnp.where(core == c, w_mine[x], w_other[x]) for c in range(2)]
        cols = slice(2 * x * HEAD_DIM, 2 * (x + 1) * HEAD_DIM)
        for k in range(2):
            lanes = slice(k * HEAD_DIM, (k + 1) * HEAD_DIM)
            rhs[k * cut : (k + 1) * cut, cols] = jnp.concatenate([p[:, lanes] for p in pair], axis=1)
    out[...] = lax.dot_general(
        lhs[...], rhs[...], (((1,), (1,)), ((), ())), preferred_element_type=jnp.float32
    ).astype(jnp.bfloat16)


def in_vmem(kernel, outs, scratch=(), grant=16, flops=2 * 10**10):
    one = not isinstance(outs, (list, tuple))
    shapes = [outs] if one else list(outs)
    specs = [pl.BlockSpec(memory_space=pltpu.VMEM) for _ in shapes]

    def call(*args):
        return pl.pallas_call(
            kernel,
            out_shape=shapes[0] if one else shapes,
            in_specs=[pl.BlockSpec(memory_space=pltpu.SMEM if a.ndim == 1 else pltpu.VMEM) for a in args],
            out_specs=specs[0] if one else specs,
            scratch_shapes=list(scratch),
            compiler_params=pltpu.CompilerParams(vmem_limit_bytes=grant and grant * 2**20),
            cost_estimate=pl.CostEstimate(flops=flops, bytes_accessed=4 * 2**20, transcendentals=0),
        )(*args)

    return call


def bias_line(table):
    far = table[:, 2 * REL_CLIP :]
    near = table[:, 1:][:, ::-1]
    heads = table.shape[0]
    return jnp.concatenate(
        [
            jnp.broadcast_to(far, (heads, REACH - REL_CLIP)),
            near,
            table[:, :1],
            jnp.broadcast_to(far, (heads, Q_BLOCK - 1)),
        ],
        axis=1,
    )


def body(tokens, documents, norm_gain, w_query, w_key, w_value, w_out, rel_bias):
    rows, width = tokens.shape
    local = w_query.shape[2]
    core = lax.axis_index("c")
    x = lax.axis_index("x")
    z = lax.axis_index(Z)
    tp = lax.axis_index("tp")
    n_tp = lax.axis_size("tp")
    plane = ("x", "c")
    group = lax.axis_size(plane)
    bf = jnp.bfloat16

    piece = w_query.shape[1]
    ids = jnp.stack([core, x, z, tp])
    sources = (w_query[0], w_key[0], w_value[0], w_out[0].T, tokens, norm_gain, documents[None, :])
    packed, block = in_vmem(
        prep_kernel,
        [
            jax.ShapeDtypeStruct((group, piece, 4 * HEAD_DIM), bf),
            jax.ShapeDtypeStruct((rows + 16, width), bf),
        ],
        grant=None,
        flops=10**9,
    )(ids, *sources)

    share = rows // n_tp
    at = lax.dynamic_slice_in_dim(tokens, tp * share, share, 0)
    line = bias_line(lax.dynamic_slice_in_dim(rel_bias[0], x * 2 + core, 1, 0))
    swap = [(0, 1), (1, 0)]
    parts = [block, lax.ppermute(block, "c", swap)]
    mine = lax.all_to_all(packed, plane, 0, 0, tiled=True)
    mine = mine.reshape(group * piece, 4 * HEAD_DIM)
    for back in (1, 2, 3):
        got = lax.ppermute(block, "x", [(i, (i + back) % 4) for i in range(4)])
        parts += [got, lax.ppermute(got, "c", swap)]
    over_far = to_all(mine, "zh")
    over_far, line, at = lax.optimization_barrier((over_far, line, at))
    near = []
    for by in (1, -1, 2):
        near.append(lax.ppermute(over_far, Z, [(n, (n + by) % 16) for n in range(16)]))
    w_in, rows_out = in_vmem(
        order_kernel,
        [
            jax.ShapeDtypeStruct((width, 4 * HEAD_DIM), bf),
            jax.ShapeDtypeStruct((width // 2, 2 * HEAD_DIM), bf),
        ],
        flops=10**9,
    )(ids, over_far, *near)
    w_mine = to_all(rows_out, "x")
    w_other = lax.ppermute(w_mine, "c", swap)
    qkv, docs, tail, head = in_vmem(
        qkv_kernel,
        [
            jax.ShapeDtypeStruct((group * rows, 4 * HEAD_DIM), bf),
            jax.ShapeDtypeStruct((group, rows), jnp.float32),
            jax.ShapeDtypeStruct((rows + 16, 4 * HEAD_DIM), bf),
            jax.ShapeDtypeStruct((rows, 4 * HEAD_DIM), bf),
        ],
        grant=24,
    )(ids, *parts, w_in)
    halo = lax.ppermute(tail, Z, [(i, i + 1) for i in range(15)])
    att_shape = jax.ShapeDtypeStruct((group, rows // 2, 2 * HEAD_DIM), bf)
    att = in_vmem(later_kernel, att_shape)(qkv, docs, line)
    att = in_vmem(early_kernel, att_shape, flops=10**9)(ids, head, halo, docs, line, att)
    att = lax.all_to_all(att, plane, 0, 0, tiled=True)
    partial = in_vmem(
        project_kernel,
        jax.ShapeDtypeStruct((rows, width), bf),
        [pltpu.VMEM((rows, local), bf), pltpu.VMEM((width, local), bf)],
    )(ids, att, w_mine, w_other)
    partial = lax.all_to_all(partial.reshape(n_tp, share, width), "tp", 0, 0, tiled=True)
    mixed = in_vmem(sum_kernel, jax.ShapeDtypeStruct((n_tp, share, width), bf), flops=10**8)(partial, at)
    return lax.all_to_all(mixed, "tp", 0, 0, tiled=True).reshape(rows, width)


def solution(mesh):
    split = Mesh(mesh.devices.reshape(4, 4, 4, 2, mesh.shape["tp"]), (*SP, "tp"))
    placed = (
        P(SP, None),
        P(SP),
        P(),
        P(None, SP, "tp"),
        P(None, SP, "tp"),
        P(None, SP, "tp"),
        P(None, None, SP),
        P(None, "tp", None),
    )

    def step(*args):
        return body(*args)

    step = jax.shard_map(step, mesh=split, in_specs=placed, out_specs=P(SP, None), check_vma=False)
    return step
```

```python
import jax
import jax.numpy as jnp
from jax import lax
from jax.experimental import pallas as pl
from jax.experimental.pallas import tpu as pltpu
from jax.sharding import Mesh
from jax.sharding import PartitionSpec as P

HEAD_DIM = 64
SEG = 64
GROUP = 14
LEFT = 4
REL_CLIP = 128
EPS = 1e-06
REACH = LEFT * SEG
Q_BLOCK = 2 * SEG
K_BLOCK = Q_BLOCK + REACH
SP = ("zh", "zl", "x", "c")
Z = ("zh", "zl")
NEG = -1e30


def to_all(x, axis):
    length = lax.axis_size(axis)
    return lax.all_to_all(jnp.broadcast_to(x[None], (length, *x.shape)), axis, 0, 0, tiled=True)


def prep_kernel(ids, w_q, w_k, w_v, w_o, tokens, gain, docs, heads, block):
    n = heads.shape[0]
    own = w_o[:, pl.ds(pl.multiple_of(ids[3] * n * HEAD_DIM, n * HEAD_DIM), n * HEAD_DIM)]
    for i in range(n):
        cols = slice(i * HEAD_DIM, (i + 1) * HEAD_DIM)
        heads[i] = jnp.concatenate([w_q[:, cols], w_k[:, cols], w_v[:, cols], own[:, cols]], axis=1)
    rows = tokens.shape[0]
    wide = tokens[...].astype(jnp.float32)
    scale = lax.rsqrt(jnp.mean(wide * wide, axis=1, keepdims=True) + EPS)
    block[:rows, :] = (wide * scale * gain[...]).astype(jnp.bfloat16)
    extra = block.shape[0] - rows
    block[rows:, :rows] = jnp.broadcast_to(docs[...].astype(jnp.float32), (extra, rows)).astype(jnp.bfloat16)
    block[rows:, rows:] = jnp.zeros((extra, block.shape[1] - rows), jnp.bfloat16)


def sum_kernel(partial, tokens, out):
    total = tokens[...].astype(jnp.float32)
    for i in range(partial.shape[0]):
        total = total + partial[i].astype(jnp.float32)
    total = total.astype(jnp.bfloat16)
    for i in range(out.shape[0]):
        out[i] = total


def qkv_kernel(ids, b0, s0, b1, s1, b2, s2, b3, s3, w_in, qkv, docs, tail, head):
    rows = qkv.shape[0] // 8
    core, x = ids[0], ids[1]
    for back, pair in enumerate(((b0, s0), (b1, s1), (b2, s2), (b3, s3))):
        for c, part in zip((core, 1 - core), pair):
            at = ((x + 4 - back) & 3) * 2 + c
            total = jnp.dot(part[:rows, :], w_in[...], preferred_element_type=jnp.float32)
            qkv[pl.ds(pl.multiple_of(at * rows, rows), rows), :] = total.astype(jnp.bfloat16)
            docs[pl.ds(at, 1), :] = part[rows : rows + 16, :rows].astype(jnp.float32)[0:1]
    head[...] = qkv[:rows, :]
    tail[:rows, :] = qkv[7 * rows :, :]
    tail[rows:, :] = jnp.broadcast_to(docs[7:8, :], (16, rows)).astype(jnp.bfloat16)


def attend(blocks, ids, qkv, halo, docs, line, out):
    rows = docs.shape[1]
    flat = jnp.broadcast_to(line[...], (Q_BLOCK, line.shape[1]))
    bias = pltpu.roll(flat, 0, 1, stride=1, stride_axis=0)[:, :K_BLOCK]
    q_seg = lax.broadcasted_iota(jnp.int32, (Q_BLOCK, K_BLOCK), 0) // SEG
    k_seg = lax.broadcasted_iota(jnp.int32, (Q_BLOCK, K_BLOCK), 1) // SEG
    bias = jnp.where((k_seg >= q_seg) & (k_seg <= q_seg + LEFT), bias, NEG)
    if halo is not None:
        prior = jnp.where(ids[2] > 0, halo[rows : rows + 16, :].astype(jnp.float32)[0:1], -1.0)

    def doc_part(b):
        if b < 0:
            return prior[:, rows + b * Q_BLOCK : rows + (b + 1) * Q_BLOCK]
        at = b * Q_BLOCK % rows
        return docs[b * Q_BLOCK // rows : b * Q_BLOCK // rows + 1, at : at + Q_BLOCK]

    def row_part(b, cols):
        if b < 0:
            return halo[rows + b * Q_BLOCK : rows + (b + 1) * Q_BLOCK, cols]
        return qkv[b * Q_BLOCK : (b + 1) * Q_BLOCK, cols]

    def key_rows(b, cols):
        if b >= 2:
            return qkv[(b - 2) * Q_BLOCK : (b + 1) * Q_BLOCK, cols]
        return jnp.concatenate([row_part(i, cols) for i in range(b - 2, b + 1)], axis=0)

    for first in range(0, len(blocks), GROUP):
        group = blocks[first : first + GROUP]
        scores = []
        for b in group:
            across = jnp.broadcast_to(doc_part(b), (Q_BLOCK, Q_BLOCK)).T
            same = jnp.concatenate([across == doc_part(i) for i in range(b - 2, b + 1)], axis=1)
            product = lax.dot_general(
                qkv[b * Q_BLOCK : (b + 1) * Q_BLOCK, :HEAD_DIM],
                key_rows(b, slice(HEAD_DIM, 2 * HEAD_DIM)),
                (((1,), (1,)), ((), ())),
                preferred_element_type=jnp.float32,
            )
            scores.append(jnp.where(same, product * HEAD_DIM ** (-0.5) + bias, NEG))
        peaks = [jnp.max(s, axis=1, keepdims=True) for s in scores]
        raised = [jnp.exp(s - p) for s, p in zip(scores, peaks)]
        totals = [jnp.sum(r, axis=1, keepdims=True) for r in raised]
        mixed = [
            jnp.dot(
                r.astype(jnp.bfloat16),
                key_rows(b, slice(2 * HEAD_DIM, 3 * HEAD_DIM)),
                preferred_element_type=jnp.float32,
            )
            for b, r in zip(group, raised)
        ]
        for b, m, t in zip(group, mixed, totals):
            lane = b % 2 * HEAD_DIM
            out[b // 2, :, lane : lane + HEAD_DIM] = (m / t).astype(jnp.bfloat16)


def later_kernel(qkv, docs, line, out):
    out[0] = jnp.zeros(out.shape[1:], out.dtype)
    attend(range(2, qkv.shape[0] // Q_BLOCK), None, qkv, None, docs, line, out)


def early_kernel(ids, qkv, halo, docs, line, later, out):
    out[1:] = later[1:]
    attend(range(2), ids, qkv, halo, docs, line, out)


def order_kernel(ids, own, below, above, second, w_all, rows_out):
    lanes = own.shape[1]
    for ahead, part in ((0, own), (3, below), (1, above), (2, second)):
        for i in range(part.shape[0]):
            z = i * 4 + ((ids[2] + ahead) & 3)
            w_all[pl.ds(pl.multiple_of(z * lanes, lanes), lanes), :] = part[i]
    half = rows_out.shape[0]
    rows_out[...] = jnp.concatenate([w_all[:half, 3 * HEAD_DIM :], w_all[half:, 3 * HEAD_DIM :]], axis=1)


def project_kernel(ids, att, w_mine, w_other, out, lhs, rhs):
    half = att.shape[1]
    for i in range(att.shape[0]):
        lhs[:half, i * HEAD_DIM : (i + 1) * HEAD_DIM] = att[i, :, :HEAD_DIM]
        lhs[half:, i * HEAD_DIM : (i + 1) * HEAD_DIM] = att[i, :, HEAD_DIM:]
    core = ids[0]
    cut = w_mine.shape[1]
    for x in range(w_mine.shape[0]):
        pair = [jnp.where(core == c, w_mine[x], w_other[x]) for c in range(2)]
        cols = slice(2 * x * HEAD_DIM, 2 * (x + 1) * HEAD_DIM)
        for k in range(2):
            lanes = slice(k * HEAD_DIM, (k + 1) * HEAD_DIM)
            rhs[k * cut : (k + 1) * cut, cols] = jnp.concatenate([p[:, lanes] for p in pair], axis=1)
    out[...] = lax.dot_general(
        lhs[...], rhs[...], (((1,), (1,)), ((), ())), preferred_element_type=jnp.float32
    ).astype(jnp.bfloat16)


def in_vmem(kernel, outs, scratch=(), grant=16, flops=2 * 10**10):
    one = not isinstance(outs, (list, tuple))
    shapes = [outs] if one else list(outs)
    specs = [pl.BlockSpec(memory_space=pltpu.VMEM) for _ in shapes]

    def call(*args):
        return pl.pallas_call(
            kernel,
            out_shape=shapes[0] if one else shapes,
            in_specs=[pl.BlockSpec(memory_space=pltpu.SMEM if a.ndim == 1 else pltpu.VMEM) for a in args],
            out_specs=specs[0] if one else specs,
            scratch_shapes=list(scratch),
            compiler_params=pltpu.CompilerParams(vmem_limit_bytes=grant and grant * 2**20),
            cost_estimate=pl.CostEstimate(flops=flops, bytes_accessed=4 * 2**20, transcendentals=0),
        )(*args)

    return call


def bias_line(table):
    far = table[:, 2 * REL_CLIP :]
    near = table[:, 1:][:, ::-1]
    heads = table.shape[0]
    return jnp.concatenate(
        [
            jnp.broadcast_to(far, (heads, REACH - REL_CLIP)),
            near,
            table[:, :1],
            jnp.broadcast_to(far, (heads, Q_BLOCK - 1)),
        ],
        axis=1,
    )


def body(tokens, documents, norm_gain, w_query, w_key, w_value, w_out, rel_bias):
    rows, width = tokens.shape
    local = w_query.shape[2]
    core = lax.axis_index("c")
    x = lax.axis_index("x")
    z = lax.axis_index(Z)
    tp = lax.axis_index("tp")
    n_tp = lax.axis_size("tp")
    plane = ("x", "c")
    group = lax.axis_size(plane)
    bf = jnp.bfloat16

    piece = w_query.shape[1]
    ids = jnp.stack([core, x, z, tp])
    sources = (w_query[0], w_key[0], w_value[0], w_out[0].T, tokens, norm_gain, documents[None, :])
    packed, block = in_vmem(
        prep_kernel,
        [
            jax.ShapeDtypeStruct((group, piece, 4 * HEAD_DIM), bf),
            jax.ShapeDtypeStruct((rows + 16, width), bf),
        ],
        grant=None,
        flops=10**9,
    )(ids, *sources)

    share = rows // n_tp
    at = lax.dynamic_slice_in_dim(tokens, tp * share, share, 0)
    line = bias_line(lax.dynamic_slice_in_dim(rel_bias[0], x * 2 + core, 1, 0))
    swap = [(0, 1), (1, 0)]
    parts = [block, lax.ppermute(block, "c", swap)]
    mine = lax.all_to_all(packed, plane, 0, 0, tiled=True)
    mine = mine.reshape(group * piece, 4 * HEAD_DIM)
    for back in (1, 2, 3):
        got = lax.ppermute(block, "x", [(i, (i + back) % 4) for i in range(4)])
        parts += [got, lax.ppermute(got, "c", swap)]
    over_far = to_all(mine, "zh")
    over_far, line, at = lax.optimization_barrier((over_far, line, at))
    near = []
    for by in (1, -1, 2):
        near.append(lax.ppermute(over_far, Z, [(n, (n + by) % 16) for n in range(16)]))
    w_in, rows_out = in_vmem(
        order_kernel,
        [
            jax.ShapeDtypeStruct((width, 4 * HEAD_DIM), bf),
            jax.ShapeDtypeStruct((width // 2, 2 * HEAD_DIM), bf),
        ],
        flops=10**9,
    )(ids, over_far, *near)
    w_mine = to_all(rows_out, "x")
    w_other = lax.ppermute(w_mine, "c", swap)
    qkv, docs, tail, head = in_vmem(
        qkv_kernel,
        [
            jax.ShapeDtypeStruct((group * rows, 4 * HEAD_DIM), bf),
            jax.ShapeDtypeStruct((group, rows), jnp.float32),
            jax.ShapeDtypeStruct((rows + 16, 4 * HEAD_DIM), bf),
            jax.ShapeDtypeStruct((rows, 4 * HEAD_DIM), bf),
        ],
        grant=24,
    )(ids, *parts, w_in)
    halo = lax.ppermute(tail, Z, [(i, i + 1) for i in range(15)])
    att_shape = jax.ShapeDtypeStruct((group, rows // 2, 2 * HEAD_DIM), bf)
    att = in_vmem(later_kernel, att_shape)(qkv, docs, line)
    att = in_vmem(early_kernel, att_shape, flops=10**9)(ids, head, halo, docs, line, att)
    att = lax.all_to_all(att, plane, 0, 0, tiled=True)
    partial = in_vmem(
        project_kernel,
        jax.ShapeDtypeStruct((rows, width), bf),
        [pltpu.VMEM((rows, local), bf), pltpu.VMEM((width, local), bf)],
    )(ids, att, w_mine, w_other)
    partial = lax.all_to_all(partial.reshape(n_tp, share, width), "tp", 0, 0, tiled=True)
    mixed = in_vmem(sum_kernel, jax.ShapeDtypeStruct((n_tp, share, width), bf), flops=10**8)(partial, at)
    return lax.all_to_all(mixed, "tp", 0, 0, tiled=True).reshape(rows, width)


def solution(mesh):
    split = Mesh(mesh.devices.reshape(4, 4, 4, 2, mesh.shape["tp"]), (*SP, "tp"))
    placed = (
        P(SP, None),
        P(SP),
        P(),
        P(None, SP, "tp"),
        P(None, SP, "tp"),
        P(None, SP, "tp"),
        P(None, None, SP),
        P(None, "tp", None),
    )

    def step(*args):
        return body(*args)

    step = jax.shard_map(step, mesh=split, in_specs=placed, out_specs=P(SP, None), check_vma=False)
    return step
```
